32 devices in a mesh: sp: 16 (over z, y, x), tp: 2 (over core).
Axes of the slice: x: 2, y: 2, z: 4, core: 2. Of those that a mesh axis runs over, the one named last changes fastest.
Arguments:
- tokens: bfloat16 [16384, 2048], P(('sp', 'tp')), may hold values from -6 to 6
- norm_gain: float32 [2048], replicated, may hold values from 0.1 to 1.9
- w_query: bfloat16 [2048, 1024], P('sp', 'tp'), may hold values from -0.125 to 0.125
- w_key: bfloat16 [2048, 1024], P('sp', 'tp'), may hold values from -0.125 to 0.125
- w_value: bfloat16 [2048, 1024], P('sp', 'tp'), may hold values from -0.125 to 0.125
- decay_rate: float32 [128, 8], P('sp', 'tp'), may hold values from 3.0517578e-06 to 0.1, as said below
- state_init: float32 [8, 128, 128], P('tp'), may hold values from -48 to 48
- out_gain: float32 [1024], P('tp'), may hold values from 0.1 to 1.9
- w_out: bfloat16 [1024, 2048], P('tp', 'sp'), may hold values from -0.1875 to 0.1875
Outputs:
- mixed: bfloat16 [16384, 2048], P(('sp', 'tp'))
The draws below stay inside these ranges and needn't reach their ends.
Inputs may be any that keep to these rules, and one draw needn't show every extreme that they name: `decay_rate`: constant over each block of 128 positions.
All inputs are finite; a program needn't handle non-finite values.
Results may differ from the reference program's by a relative error of at most 0.025.
Values may be sent and summed in bfloat16 or wider, within the bound.
A program may use at most 64 MiB of HBM per device.

```python
import math
import jax
import jax.numpy as jnp
from jax import lax

D = 2048
HEADS = 8
HEAD_DIM = 128
BLOCK = 128
SEQ = 16384
RET_WIDTH = 1024
N_TP = 2


def draw_decay_rate(key, part):
    keys = jax.random.split(key, 4)
    count_blocks = SEQ // BLOCK
    fast_share = 0.5
    fast_heads = jax.random.uniform(keys[0], (HEADS,), jnp.float32) < fast_share
    slow_base = math.log(10.0) / SEQ * jnp.exp(jax.random.uniform(keys[1], (HEADS,), jnp.float32, math.log(0.15), math.log(0.5)))
    fast_base = jnp.exp(jax.random.uniform(keys[2], (HEADS,), jnp.float32, math.log(1.0 / 50.0), math.log(1.0 / 25.0)))
    factor = jnp.exp(jax.random.uniform(keys[3], (count_blocks, HEADS), jnp.float32, math.log(0.5), math.log(2.0)))
    return (jnp.where(fast_heads, fast_base, slow_base)[None, :] * factor).astype(jnp.float32)


def level_of(key, extent, pieces, smallest, high):
    def one(position, parts):
        draws = jax.random.uniform(jax.random.fold_in(jax.random.fold_in(key, 6), position), (parts,), jnp.float32, smallest / len(pieces), high / len(pieces))
        return jnp.repeat(jnp.exp(draws), extent[position] // parts).reshape((-1,) + (1,) * (len(extent) - position - 1))

    gain = one(*pieces[0])
    for cut in pieces[1:]:
        gain = gain * one(*cut)
    return gain


def scatter_about(key, shape, deviation, bound, cuts=(), kind=jnp.bfloat16):
    entries = jax.random.normal(key, shape, jnp.float32) * deviation
    if len(cuts) > 0:
        entries = level_of(key, shape, cuts, -0.22, 0.18) * entries
    return jnp.clip(entries, min=-bound, max=bound).astype(kind)


def setup_inputs(seed: int = 0) -> dict:
    seeds = jax.random.split(jax.random.key(seed), 10)
    tokens = scatter_about(seeds[0], (SEQ, D), 1.0, 6.0, ((0, 32),))
    norm_gain = jnp.clip(1.0 + 0.18 * jax.random.normal(seeds[1], (D,), jnp.float32), 0.1, 1.9)
    w_query = scatter_about(seeds[2], (D, RET_WIDTH), D ** -0.5, 0.125, ((0, 16), (1, 2)))
    w_key = scatter_about(seeds[3], (D, RET_WIDTH), D ** -0.5, 0.125, ((0, 16), (1, 2)))
    w_value = scatter_about(seeds[4], (D, RET_WIDTH), D ** -0.5, 0.125, ((0, 16), (1, 2)))
    decay_rate = draw_decay_rate(jax.random.fold_in(seeds[9], 71), 0)
    state_init = scatter_about(seeds[6], (HEADS, HEAD_DIM, HEAD_DIM), 8.0, 48.0, ((0, 2),), jnp.float32)
    out_gain = jnp.clip(1.0 + 0.18 * jax.random.normal(seeds[7], (RET_WIDTH,), jnp.float32), 0.1, 1.9)
    w_out = scatter_about(seeds[8], (RET_WIDTH, D), RET_WIDTH ** -0.5, 0.1875, ((0, 2), (1, 16)))
    return {"tokens": tokens, "norm_gain": norm_gain, "w_query": w_query, "w_key": w_key, "w_value": w_value, "decay_rate": decay_rate, "state_init": state_init, "out_gain": out_gain, "w_out": w_out}


EPS = 0.1
ROPE_BASE = 10000.0

def rotate(values_in, positions):
    half_dim = values_in.shape[-1] // 2
    inv_freq = ROPE_BASE ** (-jnp.arange(half_dim, dtype=jnp.float32) / half_dim)
    angles = positions[:, None] * inv_freq[None, :]
    cosine = jnp.cos(angles)[:, None, :]
    sine_part = jnp.sin(angles)[:, None, :]
    first_half = values_in[..., :half_dim]
    second_half = values_in[..., half_dim:]
    return jnp.concatenate([first_half * cosine - second_half * sine_part, second_half * cosine + first_half * sine_part], axis=-1)

def reference(tokens, norm_gain, w_query, w_key, w_value, decay_rate, state_init, out_gain, w_out):
    high = lax.Precision.HIGHEST
    values_in = tokens.astype(jnp.float32)
    normed = (values_in * lax.rsqrt(lax.optimization_barrier(jnp.mean(values_in * values_in, axis=-1, keepdims=True)) + EPS) * norm_gain).astype(jnp.bfloat16)
    positions = jnp.arange(SEQ, dtype=jnp.float32)
    query_rot = rotate(jnp.dot(normed, w_query, preferred_element_type=jnp.float32).reshape(SEQ, HEADS, HEAD_DIM), positions).astype(jnp.bfloat16)
    key_rot = rotate(jnp.dot(normed, w_key, preferred_element_type=jnp.float32).reshape(SEQ, HEADS, HEAD_DIM), positions).astype(jnp.bfloat16)
    value_rows = jnp.dot(normed, w_value, preferred_element_type=jnp.float32).astype(jnp.bfloat16)
    value_rows = value_rows.reshape(SEQ, HEADS, HEAD_DIM)
    count_blocks = SEQ // BLOCK
    q_blocks = query_rot.astype(jnp.float32).reshape(count_blocks, BLOCK, HEADS, HEAD_DIM)
    k_blocks = key_rot.astype(jnp.float32).reshape(count_blocks, BLOCK, HEADS, HEAD_DIM) * HEAD_DIM ** (-0.5)
    v_blocks = value_rows.astype(jnp.float32).reshape(count_blocks, BLOCK, HEADS, HEAD_DIM)
    offsets = jnp.arange(BLOCK, dtype=jnp.float32)
    step_gap = offsets[:, None] - offsets[None, :]

    def advance(state_now, block_item):
        q_one, k_one, v_one, rate_one = block_item
        inside = jnp.where(step_gap[None] >= 0.0, jnp.exp(-jnp.maximum(step_gap, 0.0)[None] * rate_one[:, None, None]), 0.0)
        scores = jnp.einsum('ihd,jhd->hij', q_one, k_one, precision=high) * inside
        inner_part = jnp.einsum('hij,jhe->ihe', scores, v_one, precision=high)
        read_decay = jnp.exp(-(offsets + 1.0)[:, None] * rate_one[None, :])
        cross_part = jnp.einsum('ihd,hde->ihe', q_one, state_now, precision=high) * read_decay[:, :, None]
        tail_decay = jnp.exp(-(BLOCK - 1.0 - offsets)[:, None] * rate_one[None, :])
        block_kv = jnp.einsum('jhd,jhe->hde', k_one * tail_decay[:, :, None], v_one, precision=high)
        state_next = jnp.exp(-BLOCK * rate_one)[:, None, None] * state_now + block_kv
        return (state_next, inner_part + cross_part)
    final_state, retained = lax.scan(advance, state_init.astype(jnp.float32), (q_blocks, k_blocks, v_blocks, decay_rate))
    out_heads = retained.reshape(SEQ, HEADS, HEAD_DIM)
    out_heads = out_heads * lax.rsqrt(lax.optimization_barrier(jnp.mean(out_heads * out_heads, axis=-1, keepdims=True)) + EPS)
    out_heads = out_heads * out_gain.reshape(HEADS, HEAD_DIM)
    hidden = out_heads.reshape(SEQ, RET_WIDTH).astype(jnp.bfloat16)
    group_cols = RET_WIDTH // N_TP
    total_sum = jnp.zeros((SEQ, D), jnp.float32)
    for group in range(N_TP):
        partial_value = jnp.dot(hidden[:, group * group_cols:(group + 1) * group_cols], w_out[group * group_cols:(group + 1) * group_cols], preferred_element_type=jnp.float32).astype(jnp.bfloat16)
        partial_value = lax.optimization_barrier(partial_value)
        total_sum = total_sum + partial_value.astype(jnp.float32)
    return total_sum.astype(jnp.bfloat16)
```

```python
import functools

import jax
import jax.numpy as jnp
import numpy as np
from jax import lax
from jax.experimental import pallas as pl
from jax.experimental.pallas import tpu as pltpu
from jax.sharding import PartitionSpec as P

HEAD_DIM = 128
BLOCK = 128
EPS = 0.1
ROPE_BASE = 10000.0
MESH = pl.DeviceIdType.MESH
F32 = jnp.float32
BF16 = jnp.bfloat16


def remote(src, dst, send, recv, device):
    return pltpu.make_async_remote_copy(
        src_ref=src, dst_ref=dst, send_sem=send, recv_sem=recv, device_id=device, device_id_type=MESH
    )


class Gather:
    def __init__(self, buf, layers, place, sems):
        self.buf, self.layers, self.place = buf, layers, place
        self.z, self.y, self.x, self.tp = place
        self.rows = buf.shape[0] // (4 * layers)
        self.r_x, self.r_y, self.r_z, self.r_w, self.sent = sems
        self.inner = (self.z > 0) & (self.z < layers - 1)

    def at(self, zi, yi, xi, piece=None):
        start = ((zi * 2 + yi) * 2 + xi) * self.rows
        if piece is None:
            return self.buf.at[pl.ds(pl.multiple_of(start, self.rows), self.rows)]
        half = self.rows // 2
        return self.buf.at[pl.ds(pl.multiple_of(start + piece * half, half), half)]

    def device(self, zi, yi, xi):
        return ((zi * 2 + yi) * 2 + xi, self.tp)

    def layer(self, t):
        zi, bit = self.z, 1
        while bit < self.layers:
            if t & bit:
                zi = zi + bit - 2 * bit * ((self.z // bit) % 2)
            bit *= 2
        return zi

    def copy_x(self, t, j):
        ref = self.at(self.layer(t), 1 - self.y if j == 2 else self.y, self.x, (0, 1, 0, None)[j])
        return remote(ref, ref, self.sent.at[0], self.r_x.at[t // 2, j],
                      self.device(self.z, self.y, 1 - self.x))

    def copy_y(self, t, j):
        ref = self.at(self.layer(t), self.y, 1 - self.x if j == 2 else self.x, (1, 0, 1, None)[j])
        return remote(ref, ref, self.sent.at[0], self.r_y.at[t // 2, j],
                      self.device(self.z, 1 - self.y, self.x))

    def copy_w(self, t, j):
        ref = self.at(self.layer(t), 1 - self.y, 1 - self.x, j)
        return remote(ref, ref, self.sent.at[0], self.r_w.at[t // 2, j],
                      self.device(self.layer(1), self.y, self.x))

    def copy_z(self, zi, step):
        ref = self.at(zi, self.y, self.x)
        return remote(ref, ref, self.sent.at[1], self.r_z.at[zi],
                      self.device(self.z + step, self.y, self.x))

    def order(self, t):
        z, last = self.z, self.layers - 1
        near = z - (t + 1) // 2 if t % 2 else z + t // 2
        m = jnp.minimum(z, last - z)
        far = jnp.where(z < last - z, t, last - t)
        return jnp.where(t <= 2 * m, near, far)

    def along(self, zi, act):
        @pl.when((zi <= self.z) & (self.z < self.layers - 1))
        def _():
            act(self.copy_z(zi, 1))

        @pl.when((zi >= self.z) & (self.z > 0))
        def _():
            act(self.copy_z(zi, -1))

    def lead(self):
        self.along(self.z, lambda copy: copy.start())

    def take(self, t, when=None):
        zi = self.order(t)

        def go():
            self.copy_z(zi, 1).wait_recv()
            self.along(zi, lambda copy: copy.start())

        go() if when is None else pl.when(when)(go)

    def stage(self, s):
        if self.layers != 4:
            if s == 1:
                for t in range(1, self.layers):
                    self.take(t)
            return
        if s == 1:
            self.take(1)
            self.take(2, self.inner)
        elif s == 2:
            self.take(2, jnp.logical_not(self.inner))
            self.take(3, self.inner)
        else:
            self.take(3, jnp.logical_not(self.inner))

    def spread(self, t):
        if t % 2:
            self.copy_x(t, 3).start()
            self.copy_y(t, 3).start()
            return
        self.copy_y(t, 1).start()
        self.copy_x(t, 1).start()
        self.copy_x(t, 0).start()
        self.copy_y(t, 0).start()

    def cross(self, t):
        self.copy_y(t, 1).wait_recv()
        self.copy_x(t, 2).start()
        self.copy_x(t, 1).wait_recv()
        self.copy_y(t, 2).start()

    def swap(self, t):
        self.copy_x(t, 2).wait_recv()
        self.copy_w(t, 0).start()
        self.copy_y(t, 2).wait_recv()
        self.copy_w(t, 1).start()

    def arrive(self, t):
        if t % 2:
            self.copy_x(t, 3).wait_recv()
            self.copy_y(t, 3).wait_recv()
            self.copy_w(t - 1, 0).wait_recv()
            self.copy_w(t - 1, 1).wait_recv()
        else:
            self.copy_x(t, 0).wait_recv()
            self.copy_y(t, 0).wait_recv()
        return self.layer(t)

    def drain(self):
        def sent(k, shards):
            ref = self.buf.at[pl.ds(0, shards * self.rows)]
            remote(ref, ref, self.sent.at[k], self.r_z.at[0], self.device(self.z, self.y, 1 - self.x)).wait_send()

        sent(0, 3 * self.layers)
        pl.when(self.inner)(lambda: sent(1, self.layers + 1))
        pl.when(jnp.logical_not(self.inner))(lambda: sent(1, 1))


def nt_dot(a, b):
    return lax.dot_general(a, b, (((1,), (1,)), ((), ())), preferred_element_type=F32)


def tn_dot(a, b):
    return lax.dot_general(a, b, (((0,), (0,)), ((), ())), preferred_element_type=F32)


SCOPE = jax.named_scope


def kernel(layers, peers, tokens, gain_in, wq, wk, wv, wo, rates_in, state_in, out_gain_in, freq_in, out,
           gain, rates, state_init, out_gain, freq, small_sem, wkv_all, wq_all, wo_all, wo_own, toks, normed, acc, cosine, sine, q_rot, k_rot, v_row, weigh, inner,
           prev, state, hidden, part, landed, tot_send, tot_recv, excl, excl_d, pl_send, pl_recv,
           in_send, in_recv, start, incoming, local_sem, tok_sem, nrm_s, nrm_r, part_s, part_r, t_s, t_r,
           p_s, p_r, i_s, i_r,
           *gather_sems):
    me, tp = lax.axis_index("sp"), lax.axis_index("tp")
    z, y, x = me // 4, (me // 2) % 2, me % 2
    rows_here, width = tokens.shape
    span = rows_here * peers
    cols = wq.shape[1]
    heads = cols // HEAD_DIM
    blocks = span // BLOCK
    shard = wq.shape[0]
    place = (z, y, x, tp)
    gk = Gather(wkv_all, layers, place, gather_sems[:5])
    gq = Gather(wq_all, layers, place, gather_sems[5:10])
    go = Gather(wo_all, layers, place, gather_sems[10:])
    parts = nrm_s.shape[1]
    chunk = rows_here // parts

    mine = pl.ds(pl.multiple_of(me * shard, shard), shard)
    fills = [
        pltpu.make_async_copy(src, dst, local_sem.at[i])
        for i, (src, dst) in enumerate((
            (wk, wkv_all.at[mine, pl.ds(0, cols)]),
            (wv, wkv_all.at[mine, pl.ds(cols, cols)]),
            (wq, wq_all.at[mine]),
            (wo, wo_own),
        ))
    ]
    loads = [
        pltpu.make_async_copy(tokens.at[pl.ds(c * chunk, chunk)], toks.at[pl.ds(c * chunk, chunk)],
                              tok_sem.at[c])
        for c in range(parts)
    ]
    smalls = [
        pltpu.make_async_copy(src, dst, small_sem.at[i])
        for i, (src, dst) in enumerate((
            (gain_in, gain), (freq_in, freq), (rates_in, rates), (out_gain_in, out_gain),
            (state_in, state_init)))
    ]
    barrier = pltpu.get_barrier_semaphore()

    def greet(device):
        pl.semaphore_signal(barrier, inc=1, device_id=device, device_id_type=MESH)

    greet(gq.device(z, y, 1 - x))
    greet(gq.device(z, 1 - y, x))
    greet(gq.device(z, 1 - y, 1 - x))
    for d in range(1, peers):
        greet((me, (tp + d) % peers))
    for k in range(1, layers):
        pl.when(z + k < layers)(lambda: greet(gq.device(z + k, y, x)))
        pl.when(z >= k)(lambda: greet(gq.device(z - k, y, x)))

    for copy in fills + loads + smalls:
        copy.start()

    out_shard = wo.shape[1]
    for fill in fills[:3]:
        fill.wait()
    with SCOPE("barrier"):
        pl.semaphore_wait(barrier, 1 + peers + layers)

    gk.lead()
    gk.spread(0)
    gq.lead()

    base = pl.multiple_of(tp * rows_here, rows_here)
    tile = min(64, chunk)

    def send_normed(d, c):
        ref = normed.at[pl.ds(pl.multiple_of(base + c * chunk, chunk), chunk)]
        return remote(ref, ref, nrm_s.at[d - 1, c], nrm_r.at[d - 1, c], (me, (tp + d) % peers))

    for copy in smalls:
        copy.wait()
    for c in range(parts):
        loads[c].wait()

        @pl.loop(c * chunk // tile, (c + 1) * chunk // tile)
        def _(i):
            at = pl.ds(pl.multiple_of(i * tile, tile), tile)
            u = toks[at, :].astype(F32)
            scale = lax.rsqrt(jnp.mean(u * u, axis=-1, keepdims=True) + EPS)
            normed[pl.ds(pl.multiple_of(base + i * tile, tile), tile), :] = (
                u * scale * gain[...]
            ).astype(BF16)

        for d in range(1, peers):
            send_normed(d, c).start()

    fills[3].wait()
    wo_all[pl.ds(pl.multiple_of(me * out_shard, out_shard), out_shard), :] = wo_own[...].T

    def trig(i, carry):
        at = pl.ds(pl.multiple_of(i * BLOCK, BLOCK), BLOCK)
        pos = lax.broadcasted_iota(jnp.int32, (BLOCK, HEAD_DIM), 0) + (me * span + i * BLOCK)
        angle = pos.astype(F32) * freq[...]
        lane = lax.broadcasted_iota(jnp.int32, (BLOCK, HEAD_DIM), 1)
        sin = jnp.sin(angle)
        cosine[at, :] = jnp.cos(angle)
        sine[at, :] = jnp.where(lane < HEAD_DIM // 2, -sin, sin)
        return carry

    deep = 4 * shard
    m_tile = min(256, span)

    def product(gather, t, n, first, count):
        with SCOPE("arrive"):
            for i in range(n):
                zi = gather.arrive(t + i)
        at_k = pl.ds(pl.multiple_of((zi // n) * (n * deep), n * deep), n * deep)
        with SCOPE("product"):
            @pl.loop(0, span // m_tile)
            def _(i):
                at = pl.ds(pl.multiple_of(i * m_tile, m_tile), m_tile)
                for c in range(count):
                    term = jnp.dot(normed[at, at_k], gather.buf[at_k, c * cols:(c + 1) * cols],
                                   preferred_element_type=F32)
                    at_c = pl.ds((first + c) * cols, cols)
                    acc[at, at_c] = term if t == 0 else acc[at, at_c] + term

    gap = (lax.broadcasted_iota(jnp.int32, (BLOCK, BLOCK), 0)
           - lax.broadcasted_iota(jnp.int32, (BLOCK, BLOCK), 1)).astype(F32)
    row = lax.broadcasted_iota(jnp.int32, (BLOCK, HEAD_DIM), 0).astype(F32)

    def states(b, sums):
        at = pl.ds(pl.multiple_of(b * BLOCK, BLOCK), BLOCK)
        cos, sin = cosine[at, :], sine[at, :]
        new = []
        for h in range(heads):
            rate = rates[h, b]
            head = pl.ds(h * HEAD_DIM, HEAD_DIM)
            u = acc[at, pl.ds(cols + h * HEAD_DIM, HEAD_DIM)]
            k = (u * cos + pltpu.roll(u, HEAD_DIM // 2, 1) * sin).astype(BF16)
            v = acc[at, pl.ds(2 * cols + h * HEAD_DIM, HEAD_DIM)].astype(BF16)
            k_rot[at, head] = k
            v_row[at, head] = v
            tail = jnp.exp(-(BLOCK - 1.0 - row) * rate) * HEAD_DIM ** (-0.5)
            kv = tn_dot((k.astype(F32) * tail).astype(BF16), v)
            now = state[h]
            prev[b, h] = now
            state[h] = jnp.exp(jnp.full((1, HEAD_DIM), -float(BLOCK), F32) * rate) * now + kv
            new.append(sums[h] + rate)
        return tuple(new)

    def decay_of(total):
        return jnp.exp(jnp.full((1, HEAD_DIM), -float(BLOCK), F32) * total)

    corner = 2 * y + x
    slots = max(heads // 4, 1)
    owner = None if heads >= 4 else corner < heads

    def toward(r):
        return (y + r // 2 - 2 * y * (r // 2)) * 2 + (x + r % 2 - 2 * x * (r % 2))

    def guard(r, act):
        act() if heads >= 4 else pl.when(toward(r) < heads)(act)

    def beside(r):
        return (4 * z + toward(r), tp)

    def total_to(r, i):
        return remote(tot_send.at[4 * i + toward(r)], tot_recv.at[i, r], t_s.at[i, r], t_r.at[i, r], beside(r))

    def plane_to(k, i):
        return remote(pl_send.at[i], pl_recv.at[i, z], p_s.at[i, k], p_r.at[i, z], (4 * (z + k) + corner, tp))

    def plane_from(zz, i):
        return remote(pl_send.at[i], pl_recv.at[i, zz], p_s.at[i, 0], p_r.at[i, zz], (4 * z + corner, tp))

    def start_to(r, i):
        return remote(in_send.at[i, r], in_recv.at[i, r], i_s.at[i, r], i_r.at[i, r], beside(r))

    def packed(decay, value):
        return jnp.concatenate([value, jnp.broadcast_to(decay, (16, HEAD_DIM))], axis=0).astype(BF16)

    def opened(ref):
        return ref[HEAD_DIM:, :].astype(F32)[:1], ref[:HEAD_DIM, :].astype(F32)

    def mine_only(act):
        act() if heads >= 4 else pl.when(owner)(act)

    def send_totals():
        for h in range(heads):
            tot_send[h] = packed(decay_of(sums[h]), state[h])
        for r in (3, 1, 2):
            def go_out():
                for i in range(slots):
                    total_to(r, i).start()
            guard(r, go_out)

    def plane_totals():
        def act():
            for i in range(slots):
                tot_recv[i, 0] = tot_send[4 * i + corner]
                for r in (1, 2, 3):
                    total_to(r, i).wait_recv()
                decay, value = jnp.ones((1, HEAD_DIM), F32), jnp.zeros((HEAD_DIM, HEAD_DIM), F32)
                for j in range(4):
                    excl[i, j], excl_d[i, j] = value, jnp.broadcast_to(decay, (8, HEAD_DIM))
                    d, v = opened(tot_recv.at[i, toward(j)])
                    decay, value = decay * d, value * d + v
                pl_send[i] = packed(decay, value)
                for k in range(1, layers):
                    @pl.when(z + k < layers)
                    def _():
                        plane_to(k, i).start()
        mine_only(act)

    def starts():
        def act():
            for i in range(slots):
                start[...] = state_init[4 * i + corner]
                for zz in range(layers - 1):
                    @pl.when(zz < z)
                    def _():
                        plane_from(zz, i).wait_recv()
                        d, v = opened(pl_recv.at[i, zz])
                        start[...] = start[...] * d + v
                for r in (3, 1, 2):
                    at = toward(r)
                    in_send[i, r] = (excl_d[i, at][:1] * start[...] + excl[i, at]).astype(BF16)
                    start_to(r, i).start()
                incoming[4 * i + corner] = excl_d[i, corner][:1] * start[...] + excl[i, corner]
        mine_only(act)

    def started():
        for i in range(slots):
            for r in (1, 2, 3):
                def act():
                    start_to(r, i).wait_recv()
                    incoming[4 * i + toward(r)] = in_recv[i, r].astype(F32)
                guard(r, act)

    def sent_states():
        for i in range(slots):
            for r in (1, 2, 3):
                guard(r, total_to(r, i).wait_send)

            def act():
                for r in (1, 2, 3):
                    start_to(r, i).wait_send()
                for k in range(1, layers):
                    pl.when(z + k < layers)(plane_to(k, i).wait_send)
            mine_only(act)

    def turn(b, carry):
        at = pl.ds(pl.multiple_of(b * BLOCK, BLOCK), BLOCK)
        cos, sin = cosine[at, :], sine[at, :]
        for h in range(heads):
            head = pl.ds(h * HEAD_DIM, HEAD_DIM)
            u = acc[at, head]
            q_rot[at, head] = (u * cos + pltpu.roll(u, HEAD_DIM // 2, 1) * sin).astype(BF16)
        return carry

    def scores(b):
        at = pl.ds(pl.multiple_of(b * BLOCK, BLOCK), BLOCK)
        for h in range(heads):
            head = pl.ds(h * HEAD_DIM, HEAD_DIM)
            fall = jnp.where(gap >= 0.0, jnp.exp(-jnp.maximum(gap, 0.0) * rates[h, b]), 0.0)
            score = nt_dot(q_rot[at, head], k_rot[at, head]) * (fall * HEAD_DIM ** (-0.5))
            weigh[at, head] = score.astype(BF16)

    def gathered(b):
        at = pl.ds(pl.multiple_of(b * BLOCK, BLOCK), BLOCK)
        for h in range(heads):
            head = pl.ds(h * HEAD_DIM, HEAD_DIM)
            inner[at, head] = jnp.dot(weigh[at, head], v_row[at, head], preferred_element_type=F32)

    def inside(b, carry):
        gathered(b - 1)
        scores(b)
        return carry

    def finish(b, sums):
        at = pl.ds(pl.multiple_of(b * BLOCK, BLOCK), BLOCK)
        new = []
        for h in range(heads):
            rate = rates[h, b]
            head = pl.ds(h * HEAD_DIM, HEAD_DIM)
            before = prev[b, h] + decay_of(sums[h]) * incoming[h]
            read = jnp.exp(-(row + 1.0) * rate)
            kept = inner[at, head] + read * jnp.dot(
                q_rot[at, head], before.astype(BF16), preferred_element_type=F32)
            kept = kept * lax.rsqrt(jnp.mean(kept * kept, axis=-1, keepdims=True) + EPS)
            hidden[at, head] = (kept * out_gain[:, head]).astype(BF16)
            new.append(sums[h] + rate)
        return tuple(new)

    wide = 4 * out_shard
    o_tile = min(512, rows_here)

    def hand(d, t):
        return remote(part.at[d - 1, t], landed.at[d - 1, t], part_s.at[d - 1, t], part_r.at[d - 1, t],
                      (me, (tp + d) % peers))

    def pieces(t):
        with SCOPE("oarrive"):
            zi = go.arrive(t)
        return pl.ds(pl.multiple_of(zi * wide, wide), wide)

    def theirs(t):
        rows_o = pieces(t)
        with SCOPE("theirs"):
            for d in range(1, peers):
                @pl.loop(0, rows_here // o_tile)
                def _(i):
                    start = ((tp + d) % peers) * rows_here
                    rows = pl.ds(pl.multiple_of(start + i * o_tile, o_tile), o_tile)
                    part[d - 1, t, pl.ds(pl.multiple_of(i * o_tile, o_tile), o_tile), :] = nt_dot(
                        hidden[rows, :], wo_all[rows_o, :]).astype(BF16)

                hand(d, t).start()

    def ours(t):
        at_c = pl.ds(pl.multiple_of(go.layer(t) * wide, wide), wide)
        with SCOPE("w_hand"):
            for d in range(1, peers):
                hand(d, t).wait_recv()
        with SCOPE("ours"):
            @pl.loop(0, rows_here // o_tile)
            def _(i):
                at = pl.ds(pl.multiple_of(i * o_tile, o_tile), o_tile)
                rows = pl.ds(pl.multiple_of(base + i * o_tile, o_tile), o_tile)
                value = nt_dot(hidden[rows, :], wo_all[at_c, :])
                for d in range(1, peers):
                    value = value + landed[d - 1, t, at, :].astype(F32)
                out[at, at_c] = value.astype(BF16)

    def sc(name, fn, *args):
        with SCOPE(name):
            fn(*args)

    early = range(1, layers - 2 if layers > 4 else 2)
    evens = range(2, layers, 2)
    sc("kcross0", gk.cross, 0)
    sc("trig", lambda: lax.fori_loop(0, blocks // 2, trig, 0))
    sc("kstage1", gk.stage, 1)
    for t in early:
        gk.spread(t)
    gq.spread(0)
    sc("trig", lambda: lax.fori_loop(blocks // 2, blocks, trig, 0))
    with SCOPE("nrmwait"):
        for d in range(1, peers):
            for c in range(parts):
                send_normed(d, c).wait_recv()
    sc("qstage1", gq.stage, 1)
    if layers > 2:
        sc("kstage2", gk.stage, 2)
        gk.spread(layers - 2)
    sc("kswap0", gk.swap, 0)
    for t in evens:
        sc("kcross2", gk.cross, t)
    if layers > 2:
        sc("kstage3", gk.stage, 3)
        gk.spread(layers - 1)
    for t in evens:
        sc("kswap2", gk.swap, t)
    if layers > 2:
        sc("qstage2", gq.stage, 2)
        gq.spread(layers - 2)
    sc("qcross0", gq.cross, 0)
    for t in early:
        gq.spread(t)
    product(gk, 0, 2, 1, 2)
    for t in evens:
        product(gk, t, 1, 1, 2)
        product(gk, t + 1, 1, 1, 2)

    for h in range(heads):
        state[h] = jnp.zeros((HEAD_DIM, HEAD_DIM), F32)
    with SCOPE("states"):
        sums = lax.fori_loop(0, blocks, states, (jnp.float32(0.0),) * heads)
    sc("send_tot", send_totals)
    for t in evens:
        sc("qcross2", gq.cross, t)
    go.lead()
    sc("qswap0", gq.swap, 0)
    if layers > 2:
        sc("qstage3", gq.stage, 3)
        gq.spread(layers - 1)
    go.spread(0)
    sc("plane_tot", plane_totals)
    for t in evens:
        sc("qswap2", gq.swap, t)
    sc("ostage1", go.stage, 1)
    product(gq, 0, 2, 0, 1)
    sc("ocross0", go.cross, 0)
    if layers > 2:
        sc("ostage2", go.stage, 2)
        go.spread(layers - 2)
    for t in early:
        go.spread(t)
    sc("starts", starts)
    for t in evens:
        product(gq, t, 2, 0, 1)
    cut = [max(1, blocks * i // 4) for i in range(5)]
    with SCOPE("turn"):
        lax.fori_loop(0, blocks, turn, 0)
    scores(0)
    sc("oswap0", go.swap, 0)
    with SCOPE("inside"):
        lax.fori_loop(1, cut[2], inside, 0)
    if layers > 2:
        sc("ostage3", go.stage, 3)
    for t in evens:
        sc("ocross2", go.cross, t)
    if layers > 2:
        go.spread(layers - 1)
    with SCOPE("inside"):
        lax.fori_loop(cut[2], blocks, inside, 0)
        gathered(blocks - 1)
    sc("started", started)
    with SCOPE("finish"):
        lax.fori_loop(0, blocks, finish, (jnp.float32(0.0),) * heads)
    for t in evens:
        sc("oswap2", go.swap, t)
    for t in range(layers + 2):
        if t < layers:
            theirs(t)
        if t >= 2:
            ours(t - 2)

    with SCOPE("drain"):
        gk.drain()
        gq.drain()
        go.drain()
        for d in range(1, peers):
            for c in range(parts):
                send_normed(d, c).wait_send()
            for t in range(layers):
                hand(d, t).wait_send()
        sent_states()


def shards(tokens, norm_gain, w_query, w_key, w_value, decay_rate, state_init, out_gain, w_out):
    n_sp, peers = lax.axis_size("sp"), lax.axis_size("tp")
    layers = n_sp // 4
    rows_here, width = tokens.shape
    span = rows_here * peers
    cols = w_query.shape[1]
    heads = cols // HEAD_DIM
    blocks = span // BLOCK
    half = HEAD_DIM // 2
    wide = 4 * w_out.shape[1]
    freq = ROPE_BASE ** (-np.arange(half, dtype=np.float64) / half)
    freq = np.concatenate([freq, freq])[None].astype(np.float32)
    vmem = pl.BlockSpec(memory_space=pltpu.VMEM)
    hbm = pl.BlockSpec(memory_space=pl.ANY)
    dma = pltpu.SemaphoreType.DMA
    others, slots = max(peers - 1, 1), max(heads // 4, 1)
    parts = 2
    gather_sems = [dma((layers // 2, 4))] * 2 + [dma((layers,)), dma((layers // 2, 2)), dma((2,))]
    v = pltpu.VMEM
    return pl.pallas_call(
        functools.partial(kernel, layers, peers),
        out_shape=jax.ShapeDtypeStruct((rows_here, width), BF16),
        in_specs=[hbm] * 10,
        out_specs=vmem,
        scratch_shapes=[
            v((1, width), F32), pltpu.SMEM((heads, blocks), F32), v((heads, HEAD_DIM, HEAD_DIM), F32),
            v((1, cols), F32), v((1, HEAD_DIM), F32), dma((5,)),
            v((width, 2 * cols), BF16), v((width, cols), BF16), v((width, cols), BF16),
            v(w_out.shape, BF16), v((rows_here, width), BF16),
            v((span, width), BF16),
            v((span, 3 * cols), F32), v((span, HEAD_DIM), F32), v((span, HEAD_DIM), F32),
            v((span, cols), BF16), v((span, cols), BF16), v((span, cols), BF16), v((span, cols), BF16),
            v((span, cols), F32), v((blocks, heads, HEAD_DIM, HEAD_DIM), F32),
            v((heads, HEAD_DIM, HEAD_DIM), F32), v((span, cols), BF16),
            v((others, layers, rows_here, wide), BF16), v((others, layers, rows_here, wide), BF16),
            v((heads, HEAD_DIM + 16, HEAD_DIM), BF16), v((slots, 4, HEAD_DIM + 16, HEAD_DIM), BF16),
            v((slots, 4, HEAD_DIM, HEAD_DIM), F32), v((slots, 4, 8, HEAD_DIM), F32),
            v((slots, HEAD_DIM + 16, HEAD_DIM), BF16), v((slots, layers, HEAD_DIM + 16, HEAD_DIM), BF16),
            v((slots, 4, HEAD_DIM, HEAD_DIM), BF16), v((slots, 4, HEAD_DIM, HEAD_DIM), BF16),
            v((HEAD_DIM, HEAD_DIM), F32), v((heads, HEAD_DIM, HEAD_DIM), F32),
            dma((4,)), dma((parts,)), dma((others, parts)), dma((others, parts)),
            dma((others, layers)), dma((others, layers)),
            dma((slots, 4)), dma((slots, 4)), dma((slots, layers)), dma((slots, layers)),
            dma((slots, 4)), dma((slots, 4)),
        ] + gather_sems * 3,
        compiler_params=pltpu.CompilerParams(
            collective_id=0, has_side_effects=True, vmem_limit_bytes=46 * 1024 * 1024),
    )(*(pltpu.with_memory_space_constraint(u, pltpu.HBM) for u in (
        tokens, norm_gain[None], w_query, w_key, w_value, w_out, decay_rate.T, state_init,
        out_gain[None], jnp.asarray(freq))))


def solution(mesh):
    in_specs = (
        P(("sp", "tp"), None),
        P(),
        P("sp", "tp"),
        P("sp", "tp"),
        P("sp", "tp"),
        P("sp", "tp"),
        P("tp", None, None),
        P("tp"),
        P("tp", "sp"),
    )
    out_specs = P(("sp", "tp"), None)
    return jax.shard_map(shards, mesh=mesh, in_specs=in_specs, out_specs=out_specs, check_vma=False)
```

```python
import functools

import jax
import jax.numpy as jnp
import numpy as np
from jax import lax
from jax.experimental import pallas as pl
from jax.experimental.pallas import tpu as pltpu
from jax.sharding import PartitionSpec as P

HEAD_DIM = 128
BLOCK = 128
EPS = 0.1
ROPE_BASE = 10000.0
MESH = pl.DeviceIdType.MESH
F32 = jnp.float32
BF16 = jnp.bfloat16


def remote(src, dst, send, recv, device):
    return pltpu.make_async_remote_copy(
        src_ref=src, dst_ref=dst, send_sem=send, recv_sem=recv, device_id=device, device_id_type=MESH
    )


class Gather:
    def __init__(self, buf, layers, place, sems, split=False):
        self.buf, self.layers, self.place = buf, layers, place
        self.pieces = (0, 1) if split else (None,)
        self.z, self.y, self.x, self.tp = place
        self.rows = buf.shape[0] // (4 * layers)
        self.r_x, self.r_y, self.r_z, self.r_w, self.sent = sems
        self.inner = (self.z > 0) & (self.z < layers - 1)

    def at(self, zi, yi, xi, piece=None):
        start = ((zi * 2 + yi) * 2 + xi) * self.rows
        if piece is None:
            return self.buf.at[pl.ds(pl.multiple_of(start, self.rows), self.rows)]
        half = self.rows // 2
        return self.buf.at[pl.ds(pl.multiple_of(start + piece * half, half), half)]

    def device(self, zi, yi, xi):
        return ((zi * 2 + yi) * 2 + xi, self.tp)

    def layer(self, t):
        zi, bit = self.z, 1
        while bit < self.layers:
            if t & bit:
                zi = zi + bit - 2 * bit * ((self.z // bit) % 2)
            bit *= 2
        return zi

    def copy_x(self, t, j):
        ref = self.at(self.layer(t), 1 - self.y if j == 2 else self.y, self.x, (0, 1, 0, None)[j])
        return remote(ref, ref, self.sent.at[0], self.r_x.at[t // 2, j],
                      self.device(self.z, self.y, 1 - self.x))

    def copy_y(self, t, j):
        ref = self.at(self.layer(t), self.y, 1 - self.x if j == 2 else self.x, (1, 0, 1, None)[j])
        return remote(ref, ref, self.sent.at[0], self.r_y.at[t // 2, j],
                      self.device(self.z, 1 - self.y, self.x))

    def copy_w(self, t, j):
        ref = self.at(self.layer(t), 1 - self.y, 1 - self.x, j)
        return remote(ref, ref, self.sent.at[0], self.r_w.at[t // 2, j],
                      self.device(self.layer(1), self.y, self.x))

    def copy_z(self, zi, step, piece):
        ref = self.at(zi, self.y, self.x, piece)
        return remote(ref, ref, self.sent.at[1], self.r_z.at[zi, piece or 0],
                      self.device(self.z + step, self.y, self.x))

    def order(self, t):
        z, last = self.z, self.layers - 1
        near = z - (t + 1) // 2 if t % 2 else z + t // 2
        m = jnp.minimum(z, last - z)
        far = jnp.where(z < last - z, t, last - t)
        return jnp.where(t <= 2 * m, near, far)

    def along(self, zi, piece):
        @pl.when((zi <= self.z) & (self.z < self.layers - 1))
        def _():
            self.copy_z(zi, 1, piece).start()

        @pl.when((zi >= self.z) & (self.z > 0))
        def _():
            self.copy_z(zi, -1, piece).start()

    def lead(self, late=None):
        for piece in self.pieces:
            if late is None or self.layers != 4:
                if not late:
                    self.along(self.z, piece)
                continue
            even, outer = self.z % 2 == 0, jnp.logical_not(self.inner)
            odd = jnp.logical_not(even)
            up = self.inner & even if late else (self.z < self.layers - 1) & (outer | odd)
            down = self.inner & odd if late else (self.z > 0) & (outer | even)
            pl.when(up)(lambda: self.copy_z(self.z, 1, piece).start())
            pl.when(down)(lambda: self.copy_z(self.z, -1, piece).start())

    def take(self, t, pieces, when=None):
        zi = self.order(t)

        def go():
            for piece in pieces:
                self.copy_z(zi, 1, piece).wait_recv()
                self.along(zi, piece)

        go() if when is None else pl.when(when)(go)

    def stage(self, s, pieces=None):
        pieces = pieces or self.pieces
        if self.layers != 4:
            if s == 1:
                for t in range(1, self.layers):
                    self.take(t, pieces)
            return
        if s == 1:
            self.take(1, pieces)
            self.take(2, pieces, self.inner)
        elif s == 2:
            self.take(2, pieces, jnp.logical_not(self.inner))
            self.take(3, pieces, self.inner)
        else:
            self.take(3, pieces, jnp.logical_not(self.inner))

    def middle(self, *order):
        if self.layers == 4:
            for t in order:
                self.take(t, self.pieces, self.inner)
        elif 1 in order:
            for t in range(1, self.layers):
                self.take(t, self.pieces)

    def outer(self, *order):
        if self.layers == 4:
            for t in order:
                self.take(t, self.pieces, jnp.logical_not(self.inner))

    def spread(self, t):
        if t % 2:
            self.copy_x(t, 3).start()
            self.copy_y(t, 3).start()
            return
        self.copy_y(t, 1).start()
        self.copy_x(t, 1).start()
        self.copy_x(t, 0).start()
        self.copy_y(t, 0).start()

    def cross(self, t):
        self.copy_y(t, 1).wait_recv()
        self.copy_x(t, 2).start()
        self.copy_x(t, 1).wait_recv()
        self.copy_y(t, 2).start()

    def swap(self, t):
        self.copy_x(t, 2).wait_recv()
        self.copy_w(t, 0).start()
        self.copy_y(t, 2).wait_recv()
        self.copy_w(t, 1).start()

    def arrive(self, t):
        if t % 2:
            self.copy_x(t, 3).wait_recv()
            self.copy_y(t, 3).wait_recv()
            self.copy_w(t - 1, 0).wait_recv()
            self.copy_w(t - 1, 1).wait_recv()
        else:
            self.copy_x(t, 0).wait_recv()
            self.copy_y(t, 0).wait_recv()
        return self.layer(t)

    def drain(self):
        def sent(k, shards):
            ref = self.buf.at[pl.ds(0, shards * self.rows)]
            remote(ref, ref, self.sent.at[k], self.r_z.at[0, 0], self.device(self.z, self.y, 1 - self.x)).wait_send()

        sent(0, 3 * self.layers)
        pl.when(self.inner)(lambda: sent(1, self.layers + 1))
        pl.when(jnp.logical_not(self.inner))(lambda: sent(1, 1))


def nt_dot(a, b):
    return lax.dot_general(a, b, (((1,), (1,)), ((), ())), preferred_element_type=F32)


def tn_dot(a, b):
    return lax.dot_general(a, b, (((0,), (0,)), ((), ())), preferred_element_type=F32)


SCOPE = jax.named_scope


def kernel(layers, peers, tokens, gain_in, wq, wk, wv, wo, rates_in, state_in, out_gain_in, freq_in, out,
           gain, rates, state_init, out_gain, freq, small_sem, wkv_all, wq_all, wo_all, wo_own, toks, normed, acc, cosine, sine, q_rot, k_rot, v_row, weigh, inner,
           prev, state, hidden, part, landed, tot_send, tot_recv, excl, excl_d, pl_send, pl_recv,
           in_send, in_recv, start, incoming, local_sem, tok_sem, nrm_s, nrm_r, part_s, part_r, t_s, t_r,
           p_s, p_r, i_s, i_r,
           *gather_sems):
    me, tp = lax.axis_index("sp"), lax.axis_index("tp")
    z, y, x = me // 4, (me // 2) % 2, me % 2
    rows_here, width = tokens.shape
    span = rows_here * peers
    cols = wq.shape[1]
    heads = cols // HEAD_DIM
    blocks = span // BLOCK
    shard = wq.shape[0]
    place = (z, y, x, tp)
    gk = Gather(wkv_all, layers, place, gather_sems[:5], True)
    gq = Gather(wq_all, layers, place, gather_sems[5:10])
    go = Gather(wo_all, layers, place, gather_sems[10:])
    parts = nrm_s.shape[1]
    chunk = rows_here // parts

    mine = pl.ds(pl.multiple_of(me * shard, shard), shard)
    fills = [
        pltpu.make_async_copy(src, dst, local_sem.at[i])
        for i, (src, dst) in enumerate((
            (wk, wkv_all.at[mine, pl.ds(0, cols)]),
            (wv, wkv_all.at[mine, pl.ds(cols, cols)]),
            (wq, wq_all.at[mine]),
            (wo, wo_own),
        ))
    ]
    loads = [
        pltpu.make_async_copy(tokens.at[pl.ds(c * chunk, chunk)], toks.at[pl.ds(c * chunk, chunk)],
                              tok_sem.at[c])
        for c in range(parts)
    ]
    smalls = [
        pltpu.make_async_copy(src, dst, small_sem.at[i])
        for i, (src, dst) in enumerate((
            (gain_in, gain), (freq_in, freq), (rates_in, rates), (out_gain_in, out_gain),
            (state_in, state_init)))
    ]
    barrier = pltpu.get_barrier_semaphore()

    def greet(device):
        pl.semaphore_signal(barrier, inc=1, device_id=device, device_id_type=MESH)

    greet(gq.device(z, y, 1 - x))
    greet(gq.device(z, 1 - y, x))
    for d in range(1, peers):
        greet((me, (tp + d) % peers))
    pl.when(z > 0)(lambda: greet(gq.device(z - 1, y, x)))
    pl.when(z < layers - 1)(lambda: greet(gq.device(z + 1, y, x)))

    for copy in fills + loads + smalls:
        copy.start()

    out_shard = wo.shape[1]
    for fill in fills[:3]:
        fill.wait()
    with SCOPE("barrier"):
        pl.semaphore_wait(
            barrier, 1 + peers + jnp.minimum(z, 1) + jnp.minimum(layers - 1 - z, 1))

    gk.lead()
    gk.spread(0)

    base = pl.multiple_of(tp * rows_here, rows_here)
    tile = min(64, chunk)

    def send_normed(d, c):
        ref = normed.at[pl.ds(pl.multiple_of(base + c * chunk, chunk), chunk)]
        return remote(ref, ref, nrm_s.at[d - 1, c], nrm_r.at[d - 1, c], (me, (tp + d) % peers))

    for copy in smalls:
        copy.wait()
    for c in range(parts):
        loads[c].wait()

        @pl.loop(c * chunk // tile, (c + 1) * chunk // tile)
        def _(i):
            at = pl.ds(pl.multiple_of(i * tile, tile), tile)
            u = toks[at, :].astype(F32)
            scale = lax.rsqrt(jnp.mean(u * u, axis=-1, keepdims=True) + EPS)
            normed[pl.ds(pl.multiple_of(base + i * tile, tile), tile), :] = (
                u * scale * gain[...]
            ).astype(BF16)

        for d in range(1, peers):
            send_normed(d, c).start()

    fills[3].wait()
    wo_all[pl.ds(pl.multiple_of(me * out_shard, out_shard), out_shard), :] = wo_own[...].T

    def trig(i, carry):
        at = pl.ds(pl.multiple_of(i * BLOCK, BLOCK), BLOCK)
        pos = lax.broadcasted_iota(jnp.int32, (BLOCK, HEAD_DIM), 0) + (me * span + i * BLOCK)
        angle = pos.astype(F32) * freq[...]
        lane = lax.broadcasted_iota(jnp.int32, (BLOCK, HEAD_DIM), 1)
        sin = jnp.sin(angle)
        cosine[at, :] = jnp.cos(angle)
        sine[at, :] = jnp.where(lane < HEAD_DIM // 2, -sin, sin)
        return carry

    deep = 4 * shard
    m_tile = min(256, span)

    def product(gather, t, n, first, count):
        with SCOPE("arrive"):
            for i in range(n):
                zi = gather.arrive(t + i)
        at_k = pl.ds(pl.multiple_of((zi // n) * (n * deep), n * deep), n * deep)
        with SCOPE("product"):
            @pl.loop(0, span // m_tile)
            def _(i):
                at = pl.ds(pl.multiple_of(i * m_tile, m_tile), m_tile)
                for c in range(count):
                    term = jnp.dot(normed[at, at_k], gather.buf[at_k, c * cols:(c + 1) * cols],
                                   preferred_element_type=F32)
                    at_c = pl.ds((first + c) * cols, cols)
                    acc[at, at_c] = term if t == 0 else acc[at, at_c] + term

    gap = (lax.broadcasted_iota(jnp.int32, (BLOCK, BLOCK), 0)
           - lax.broadcasted_iota(jnp.int32, (BLOCK, BLOCK), 1)).astype(F32)
    row = lax.broadcasted_iota(jnp.int32, (BLOCK, HEAD_DIM), 0).astype(F32)

    def states(b, sums):
        at = pl.ds(pl.multiple_of(b * BLOCK, BLOCK), BLOCK)
        cos, sin = cosine[at, :], sine[at, :]
        new = []
        for h in range(heads):
            rate = rates[h, b]
            head = pl.ds(h * HEAD_DIM, HEAD_DIM)
            u = acc[at, pl.ds(cols + h * HEAD_DIM, HEAD_DIM)]
            k = (u * cos + pltpu.roll(u, HEAD_DIM // 2, 1) * sin).astype(BF16)
            v = acc[at, pl.ds(2 * cols + h * HEAD_DIM, HEAD_DIM)].astype(BF16)
            k_rot[at, head] = k
            v_row[at, head] = v
            tail = jnp.exp(-(BLOCK - 1.0 - row) * rate) * HEAD_DIM ** (-0.5)
            kv = tn_dot((k.astype(F32) * tail).astype(BF16), v)
            now = state[h]
            prev[b, h] = now
            state[h] = jnp.exp(jnp.full((1, HEAD_DIM), -float(BLOCK), F32) * rate) * now + kv
            new.append(sums[h] + rate)
        return tuple(new)

    def decay_of(total):
        return jnp.exp(jnp.full((1, HEAD_DIM), -float(BLOCK), F32) * total)

    corner = 2 * y + x
    slots = max(heads // 4, 1)
    owner = None if heads >= 4 else corner < heads

    def toward(r):
        return (y + r // 2 - 2 * y * (r // 2)) * 2 + (x + r % 2 - 2 * x * (r % 2))

    def guard(r, act):
        act() if heads >= 4 else pl.when(toward(r) < heads)(act)

    def beside(r):
        return (4 * z + toward(r), tp)

    def total_to(r, i):
        return remote(tot_send.at[4 * i + toward(r)], tot_recv.at[i, r], t_s.at[i, r], t_r.at[i, r], beside(r))

    def plane_to(k, i):
        return remote(pl_send.at[i], pl_recv.at[i, z], p_s.at[i, k], p_r.at[i, z], (4 * (z + k) + corner, tp))

    def plane_from(zz, i):
        return remote(pl_send.at[i], pl_recv.at[i, zz], p_s.at[i, 0], p_r.at[i, zz], (4 * z + corner, tp))

    def start_to(r, i):
        return remote(in_send.at[i, r], in_recv.at[i, r], i_s.at[i, r], i_r.at[i, r], beside(r))

    def packed(decay, value):
        return jnp.concatenate([value, jnp.broadcast_to(decay, (16, HEAD_DIM))], axis=0).astype(BF16)

    def opened(ref):
        return ref[HEAD_DIM:, :].astype(F32)[:1], ref[:HEAD_DIM, :].astype(F32)

    def mine_only(act):
        act() if heads >= 4 else pl.when(owner)(act)

    def send_totals():
        for h in range(heads):
            tot_send[h] = packed(decay_of(sums[h]), state[h])
        for r in (3, 1, 2):
            def go_out():
                for i in range(slots):
                    total_to(r, i).start()
            guard(r, go_out)

    def plane_totals():
        def act():
            for i in range(slots):
                tot_recv[i, 0] = tot_send[4 * i + corner]
                for r in (1, 2, 3):
                    total_to(r, i).wait_recv()
                decay, value = jnp.ones((1, HEAD_DIM), F32), jnp.zeros((HEAD_DIM, HEAD_DIM), F32)
                for j in range(4):
                    excl[i, j], excl_d[i, j] = value, jnp.broadcast_to(decay, (8, HEAD_DIM))
                    d, v = opened(tot_recv.at[i, toward(j)])
                    decay, value = decay * d, value * d + v
                pl_send[i] = packed(decay, value)
                for k in range(1, layers):
                    @pl.when(z + k < layers)
                    def _():
                        plane_to(k, i).start()
        mine_only(act)

    def starts():
        def act():
            for i in range(slots):
                start[...] = state_init[4 * i + corner]
                for zz in range(layers - 1):
                    @pl.when(zz < z)
                    def _():
                        plane_from(zz, i).wait_recv()
                        d, v = opened(pl_recv.at[i, zz])
                        start[...] = start[...] * d + v
                for r in (3, 1, 2):
                    at = toward(r)
                    in_send[i, r] = (excl_d[i, at][:1] * start[...] + excl[i, at]).astype(BF16)
                    start_to(r, i).start()
                incoming[4 * i + corner] = excl_d[i, corner][:1] * start[...] + excl[i, corner]
        mine_only(act)

    def started():
        for i in range(slots):
            for r in (1, 2, 3):
                def act():
                    start_to(r, i).wait_recv()
                    incoming[4 * i + toward(r)] = in_recv[i, r].astype(F32)
                guard(r, act)

    def sent_states():
        for i in range(slots):
            for r in (1, 2, 3):
                guard(r, total_to(r, i).wait_send)

            def act():
                for r in (1, 2, 3):
                    start_to(r, i).wait_send()
                for k in range(1, layers):
                    pl.when(z + k < layers)(plane_to(k, i).wait_send)
            mine_only(act)

    def turn(b, carry):
        at = pl.ds(pl.multiple_of(b * BLOCK, BLOCK), BLOCK)
        cos, sin = cosine[at, :], sine[at, :]
        for h in range(heads):
            head = pl.ds(h * HEAD_DIM, HEAD_DIM)
            u = acc[at, head]
            q_rot[at, head] = (u * cos + pltpu.roll(u, HEAD_DIM // 2, 1) * sin).astype(BF16)
        return carry

    def scores(b):
        at = pl.ds(pl.multiple_of(b * BLOCK, BLOCK), BLOCK)
        for h in range(heads):
            head = pl.ds(h * HEAD_DIM, HEAD_DIM)
            fall = jnp.where(gap >= 0.0, jnp.exp(-jnp.maximum(gap, 0.0) * rates[h, b]), 0.0)
            score = nt_dot(q_rot[at, head], k_rot[at, head]) * (fall * HEAD_DIM ** (-0.5))
            weigh[at, head] = score.astype(BF16)

    def gathered(b):
        at = pl.ds(pl.multiple_of(b * BLOCK, BLOCK), BLOCK)
        for h in range(heads):
            head = pl.ds(h * HEAD_DIM, HEAD_DIM)
            inner[at, head] = jnp.dot(weigh[at, head], v_row[at, head], preferred_element_type=F32)

    def inside(b, carry):
        gathered(b - 1)
        scores(b)
        return carry

    def finish(b, sums):
        at = pl.ds(pl.multiple_of(b * BLOCK, BLOCK), BLOCK)
        new = []
        for h in range(heads):
            rate = rates[h, b]
            head = pl.ds(h * HEAD_DIM, HEAD_DIM)
            before = prev[b, h] + decay_of(sums[h]) * incoming[h]
            read = jnp.exp(-(row + 1.0) * rate)
            kept = inner[at, head] + read * jnp.dot(
                q_rot[at, head], before.astype(BF16), preferred_element_type=F32)
            kept = kept * lax.rsqrt(jnp.mean(kept * kept, axis=-1, keepdims=True) + EPS)
            hidden[at, head] = (kept * out_gain[:, head]).astype(BF16)
            new.append(sums[h] + rate)
        return tuple(new)

    wide = 4 * out_shard
    o_tile = min(512, rows_here)

    def hand(d, t):
        return remote(part.at[d - 1, t], landed.at[d - 1, t], part_s.at[d - 1, t], part_r.at[d - 1, t],
                      (me, (tp + d) % peers))

    def pieces(t):
        with SCOPE("oarrive"):
            zi = go.arrive(t)
        return pl.ds(pl.multiple_of(zi * wide, wide), wide)

    def theirs(t):
        rows_o = pieces(t)
        with SCOPE("theirs"):
            for d in range(1, peers):
                @pl.loop(0, rows_here // o_tile)
                def _(i):
                    start = ((tp + d) % peers) * rows_here
                    rows = pl.ds(pl.multiple_of(start + i * o_tile, o_tile), o_tile)
                    part[d - 1, t, pl.ds(pl.multiple_of(i * o_tile, o_tile), o_tile), :] = nt_dot(
                        hidden[rows, :], wo_all[rows_o, :]).astype(BF16)

                hand(d, t).start()

    def ours(t):
        at_c = pl.ds(pl.multiple_of(go.layer(t) * wide, wide), wide)
        with SCOPE("w_hand"):
            for d in range(1, peers):
                hand(d, t).wait_recv()
        with SCOPE("ours"):
            @pl.loop(0, rows_here // o_tile)
            def _(i):
                at = pl.ds(pl.multiple_of(i * o_tile, o_tile), o_tile)
                rows = pl.ds(pl.multiple_of(base + i * o_tile, o_tile), o_tile)
                value = nt_dot(hidden[rows, :], wo_all[at_c, :])
                for d in range(1, peers):
                    value = value + landed[d - 1, t, at, :].astype(F32)
                out[at, at_c] = value.astype(BF16)

    def sc(name, fn, *args):
        with SCOPE(name):
            fn(*args)

    evens, odds, last = range(2, layers, 2), range(1, layers - 2, 2), layers - 1
    cut = max(1, blocks // 2)

    def each(name, ts, fn):
        for t in ts:
            sc(name, fn, t)

    sc("kcross0", gk.cross, 0)
    sc("kstage1a", gk.stage, 1, (0,))
    sc("trig", lambda: lax.fori_loop(0, cut, trig, 0))
    sc("kstage1b", gk.stage, 1, (1,))
    each("kspread", odds, gk.spread)
    sc("trig", lambda: lax.fori_loop(cut, blocks, trig, 0))
    with SCOPE("nrmwait"):
        for d in range(1, peers):
            for c in range(parts):
                send_normed(d, c).wait_recv()
    sc("kstage2a", gk.stage, 2, (0,))
    sc("kstage2b", gk.stage, 2, (1,))
    each("kspread", evens, gk.spread)
    sc("kswap0", gk.swap, 0)
    gq.lead(False)
    product(gk, 0, 1, 1, 2)
    each("kcross2", evens, gk.cross)
    gq.spread(0)
    sc("kstage3", gk.stage, 3)
    gk.spread(last)
    sc("qmiddle", gq.middle, 1, 2)
    each("kswap2", evens, gk.swap)
    for t in evens:
        product(gk, t, 1, 1, 2)
    sc("qmiddle3", gq.middle, 3)
    sc("qouter2", gq.outer, 2)
    gq.lead(True)
    each("qspread", evens, gq.spread)
    for t in odds:
        product(gk, t, 1, 1, 2)
    sc("qcross0", gq.cross, 0)
    go.lead(False)
    product(gk, last, 1, 1, 2)

    for h in range(heads):
        state[h] = jnp.zeros((HEAD_DIM, HEAD_DIM), F32)
    with SCOPE("states"):
        sums = lax.fori_loop(0, cut, states, (jnp.float32(0.0),) * heads)
    each("qcross2", evens, gq.cross)
    sc("omiddle", go.middle, 1, 2)
    with SCOPE("states"):
        sums = lax.fori_loop(cut, blocks, states, sums)
    sc("send_tot", send_totals)
    sc("qswap0", gq.swap, 0)
    sc("qouter3", gq.outer, 3)
    sc("qouter1", gq.outer, 1)
    each("qspread", odds, gq.spread)
    gq.spread(last)
    each("qswap2", evens, gq.swap)
    sc("plane_tot", plane_totals)
    sc("omiddle3", go.middle, 3)
    go.lead(True)
    go.spread(0)
    product(gq, 0, 2, 0, 1)
    sc("oouter2", go.outer, 2)
    each("ospread", evens, go.spread)
    sc("starts", starts)
    for t in evens:
        product(gq, t, 2, 0, 1)
    sc("ocross0", go.cross, 0)
    with SCOPE("turn"):
        lax.fori_loop(0, blocks, turn, 0)
    scores(0)
    sc("oouter3", go.outer, 3)
    go.spread(last)
    each("ocross2", evens, go.cross)
    with SCOPE("inside"):
        lax.fori_loop(1, cut, inside, 0)
    sc("oouter1", go.outer, 1)
    each("ospread", odds, go.spread)
    sc("oswap0", go.swap, 0)
    with SCOPE("inside"):
        lax.fori_loop(cut, blocks, inside, 0)
        gathered(blocks - 1)
    sc("started", started)
    with SCOPE("finish"):
        sums = lax.fori_loop(0, cut, finish, (jnp.float32(0.0),) * heads)
    each("oswap2", evens, go.swap)
    with SCOPE("finish"):
        lax.fori_loop(cut, blocks, finish, sums)
    turns = (0,) + tuple(evens) + tuple(odds) + (last,) if layers > 2 else (0, 1)
    for i in range(layers + 2):
        if i < layers:
            theirs(turns[i])
        if i >= 2:
            ours(turns[i - 2])

    with SCOPE("drain"):
        gk.drain()
        gq.drain()
        go.drain()
        for d in range(1, peers):
            for c in range(parts):
                send_normed(d, c).wait_send()
            for t in range(layers):
                hand(d, t).wait_send()
        sent_states()


def shards(tokens, norm_gain, w_query, w_key, w_value, decay_rate, state_init, out_gain, w_out):
    n_sp, peers = lax.axis_size("sp"), lax.axis_size("tp")
    layers = n_sp // 4
    rows_here, width = tokens.shape
    span = rows_here * peers
    cols = w_query.shape[1]
    heads = cols // HEAD_DIM
    blocks = span // BLOCK
    half = HEAD_DIM // 2
    wide = 4 * w_out.shape[1]
    freq = ROPE_BASE ** (-np.arange(half, dtype=np.float64) / half)
    freq = np.concatenate([freq, freq])[None].astype(np.float32)
    vmem = pl.BlockSpec(memory_space=pltpu.VMEM)
    hbm = pl.BlockSpec(memory_space=pl.ANY)
    dma = pltpu.SemaphoreType.DMA
    others, slots = max(peers - 1, 1), max(heads // 4, 1)
    parts = 2
    gather_sems = [dma((layers // 2, 4))] * 2 + [dma((layers, 2)), dma((layers // 2, 2)), dma((2,))]
    v = pltpu.VMEM
    return pl.pallas_call(
        functools.partial(kernel, layers, peers),
        out_shape=jax.ShapeDtypeStruct((rows_here, width), BF16),
        in_specs=[hbm] * 10,
        out_specs=vmem,
        scratch_shapes=[
            v((1, width), F32), pltpu.SMEM((heads, blocks), F32), v((heads, HEAD_DIM, HEAD_DIM), F32),
            v((1, cols), F32), v((1, HEAD_DIM), F32), dma((5,)),
            v((width, 2 * cols), BF16), v((width, cols), BF16), v((width, cols), BF16),
            v(w_out.shape, BF16), v((rows_here, width), BF16),
            v((span, width), BF16),
            v((span, 3 * cols), F32), v((span, HEAD_DIM), F32), v((span, HEAD_DIM), F32),
            v((span, cols), BF16), v((span, cols), BF16), v((span, cols), BF16), v((span, cols), BF16),
            v((span, cols), F32), v((blocks, heads, HEAD_DIM, HEAD_DIM), F32),
            v((heads, HEAD_DIM, HEAD_DIM), F32), v((span, cols), BF16),
            v((others, layers, rows_here, wide), BF16), v((others, layers, rows_here, wide), BF16),
            v((heads, HEAD_DIM + 16, HEAD_DIM), BF16), v((slots, 4, HEAD_DIM + 16, HEAD_DIM), BF16),
            v((slots, 4, HEAD_DIM, HEAD_DIM), F32), v((slots, 4, 8, HEAD_DIM), F32),
            v((slots, HEAD_DIM + 16, HEAD_DIM), BF16), v((slots, layers, HEAD_DIM + 16, HEAD_DIM), BF16),
            v((slots, 4, HEAD_DIM, HEAD_DIM), BF16), v((slots, 4, HEAD_DIM, HEAD_DIM), BF16),
            v((HEAD_DIM, HEAD_DIM), F32), v((heads, HEAD_DIM, HEAD_DIM), F32),
            dma((4,)), dma((parts,)), dma((others, parts)), dma((others, parts)),
            dma((others, layers)), dma((others, layers)),
            dma((slots, 4)), dma((slots, 4)), dma((slots, layers)), dma((slots, layers)),
            dma((slots, 4)), dma((slots, 4)),
        ] + gather_sems * 3,
        compiler_params=pltpu.CompilerParams(
            collective_id=0, has_side_effects=True, vmem_limit_bytes=46 * 1024 * 1024),
    )(*(pltpu.with_memory_space_constraint(u, pltpu.HBM) for u in (
        tokens, norm_gain[None], w_query, w_key, w_value, w_out, decay_rate.T, state_init,
        out_gain[None], jnp.asarray(freq))))


def solution(mesh):
    in_specs = (
        P(("sp", "tp"), None),
        P(),
        P("sp", "tp"),
        P("sp", "tp"),
        P("sp", "tp"),
        P("sp", "tp"),
        P("tp", None, None),
        P("tp"),
        P("tp", "sp"),
    )
    out_specs = P(("sp", "tp"), None)
    return jax.shard_map(shards, mesh=mesh, in_specs=in_specs, out_specs=out_specs, check_vma=False)
```

```python
import functools

import jax
import jax.numpy as jnp
import numpy as np
from jax import lax
from jax.experimental import pallas as pl
from jax.experimental.pallas import tpu as pltpu
from jax.sharding import PartitionSpec as P

HEAD_DIM = 128
BLOCK = 128
EPS = 0.1
ROPE_BASE = 10000.0
MESH = pl.DeviceIdType.MESH
F32 = jnp.float32
BF16 = jnp.bfloat16


def remote(src, dst, send, recv, device):
    return pltpu.make_async_remote_copy(
        src_ref=src, dst_ref=dst, send_sem=send, recv_sem=recv, device_id=device, device_id_type=MESH
    )


class Gather:
    def __init__(self, buf, layers, place, sems, split=False):
        self.buf, self.layers, self.place = buf, layers, place
        self.pieces = (0, 1) if split else (None,)
        self.z, self.y, self.x, self.tp = place
        self.rows = buf.shape[0] // (4 * layers)
        self.got, self.r_z, self.sent = sems
        self.inner = (self.z > 0) & (self.z < layers - 1)

    def at(self, zi, yi, xi, piece=None):
        start = ((zi * 2 + yi) * 2 + xi) * self.rows
        if piece is None:
            return self.buf.at[pl.ds(pl.multiple_of(start, self.rows), self.rows)]
        half = self.rows // 2
        return self.buf.at[pl.ds(pl.multiple_of(start + piece * half, half), half)]

    def device(self, zi, yi, xi):
        return ((zi * 2 + yi) * 2 + xi, self.tp)

    def layer(self, t):
        zi, bit = self.z, 1
        while bit < self.layers:
            if t & bit:
                zi = zi + bit - 2 * bit * ((self.z // bit) % 2)
            bit *= 2
        return zi

    def copy_x(self, t, j):
        ref = self.at(self.layer(t), 1 - self.y if j == 2 else self.y, self.x, (0, 1, 0, None)[j])
        return remote(ref, ref, self.sent.at[0], self.got.at[t // 2, (4, 0, 2, 5)[j]],
                      self.device(self.z, self.y, 1 - self.x))

    def copy_y(self, t, j):
        ref = self.at(self.layer(t), self.y, 1 - self.x if j == 2 else self.x, (1, 0, 1, None)[j])
        return remote(ref, ref, self.sent.at[0], self.got.at[t // 2, (4, 1, 3, 5)[j]],
                      self.device(self.z, 1 - self.y, self.x))

    def copy_w(self, t, j):
        ref = self.at(self.layer(t), 1 - self.y, 1 - self.x, j)
        return remote(ref, ref, self.sent.at[0], self.got.at[t // 2, 5],
                      self.device(self.layer(1), self.y, self.x))

    def whole(self, t, shards, k):
        ref = self.buf.at[pl.ds(0, shards * self.rows)]
        remote(ref, ref, self.sent.at[0], self.got.at[t // 2, k],
               self.device(self.z, self.y, 1 - self.x)).wait_recv()

    def copy_z(self, zi, step, piece):
        ref = self.at(zi, self.y, self.x, piece)
        return remote(ref, ref, self.sent.at[1], self.r_z.at[zi, piece or 0],
                      self.device(self.z + step, self.y, self.x))

    def order(self, t):
        z, last = self.z, self.layers - 1
        near = z - (t + 1) // 2 if t % 2 else z + t // 2
        m = jnp.minimum(z, last - z)
        far = jnp.where(z < last - z, t, last - t)
        return jnp.where(t <= 2 * m, near, far)

    def along(self, zi, piece):
        @pl.when((zi <= self.z) & (self.z < self.layers - 1))
        def _():
            self.copy_z(zi, 1, piece).start()

        @pl.when((zi >= self.z) & (self.z > 0))
        def _():
            self.copy_z(zi, -1, piece).start()

    def lead(self, late=None):
        for piece in self.pieces:
            if late is None or self.layers != 4:
                if not late:
                    self.along(self.z, piece)
                continue
            even, outer = self.z % 2 == 0, jnp.logical_not(self.inner)
            odd = jnp.logical_not(even)
            up = self.inner & even if late else (self.z < self.layers - 1) & (outer | odd)
            down = self.inner & odd if late else (self.z > 0) & (outer | even)
            pl.when(up)(lambda: self.copy_z(self.z, 1, piece).start())
            pl.when(down)(lambda: self.copy_z(self.z, -1, piece).start())

    def take(self, t, pieces, when=None):
        zi = self.order(t)

        def go():
            for piece in pieces:
                self.copy_z(zi, 1, piece).wait_recv()
                self.along(zi, piece)

        go() if when is None else pl.when(when)(go)

    def stage(self, s, pieces=None):
        pieces = pieces or self.pieces
        if self.layers != 4:
            if s == 1:
                for t in range(1, self.layers):
                    self.take(t, pieces)
            return
        if s == 1:
            self.take(1, pieces)
            self.take(2, pieces, self.inner)
        elif s == 2:
            self.take(2, pieces, jnp.logical_not(self.inner))
            self.take(3, pieces, self.inner)
        else:
            self.take(3, pieces, jnp.logical_not(self.inner))

    def middle(self, *order):
        if self.layers == 4:
            for t in order:
                self.take(t, self.pieces, self.inner)
        elif 1 in order:
            for t in range(1, self.layers):
                self.take(t, self.pieces)

    def outer(self, *order):
        if self.layers == 4:
            for t in order:
                self.take(t, self.pieces, jnp.logical_not(self.inner))

    def spread(self, t):
        if t % 2:
            self.copy_x(t, 3).start()
            self.copy_y(t, 3).start()
            return
        self.copy_y(t, 1).start()
        self.copy_x(t, 1).start()
        self.copy_x(t, 0).start()
        self.copy_y(t, 0).start()

    def cross(self, t):
        self.copy_y(t, 1).wait_recv()
        self.copy_x(t, 2).start()
        self.copy_x(t, 1).wait_recv()
        self.copy_y(t, 2).start()

    def swap(self, t):
        self.copy_x(t, 2).wait_recv()
        self.copy_w(t, 0).start()
        self.copy_y(t, 2).wait_recv()
        self.copy_w(t, 1).start()

    def arrive(self, t):
        self.whole(t, 3, 5) if t % 2 else self.whole(t, 1, 4)
        return self.layer(t)

    def drain(self):
        def sent(k, shards):
            ref = self.buf.at[pl.ds(0, shards * self.rows)]
            remote(ref, ref, self.sent.at[k], self.r_z.at[0, 0], self.device(self.z, self.y, 1 - self.x)).wait_send()

        sent(0, 3 * self.layers)
        pl.when(self.inner)(lambda: sent(1, self.layers + 1))
        pl.when(jnp.logical_not(self.inner))(lambda: sent(1, 1))


def nt_dot(a, b):
    return lax.dot_general(a, b, (((1,), (1,)), ((), ())), preferred_element_type=F32)


def tn_dot(a, b):
    return lax.dot_general(a, b, (((0,), (0,)), ((), ())), preferred_element_type=F32)


SCOPE = jax.named_scope


def kernel(layers, peers, tokens, gain_in, wq, wk, wv, wo, rates_in, state_in, out_gain_in, freq_in, out,
           gain, rates, state_init, out_gain, freq, small_sem, wkv_all, wq_all, wo_all, wo_own, toks, normed, acc, cosine, sine, q_rot, k_rot, v_row, weigh,
           prev, state, hidden, part, landed, tot_send, tot_recv, excl, excl_d, pl_send, pl_recv,
           in_send, in_recv, start, incoming, local_sem, tok_sem, nrm_s, nrm_r, part_s, part_r, t_s, t_r,
           p_s, p_r, i_s, i_r,
           *gather_sems):
    me, tp = lax.axis_index("sp"), lax.axis_index("tp")
    z, y, x = me // 4, (me // 2) % 2, me % 2
    rows_here, width = tokens.shape
    span = rows_here * peers
    cols = wq.shape[1]
    heads = cols // HEAD_DIM
    blocks = span // BLOCK
    shard = wq.shape[0]
    place = (z, y, x, tp)
    gk = Gather(wkv_all, layers, place, gather_sems[:3], True)
    gq = Gather(wq_all, layers, place, gather_sems[3:6])
    go = Gather(wo_all, layers, place, gather_sems[6:])
    parts = tok_sem.shape[0]
    chunk = rows_here // parts

    mine = pl.ds(pl.multiple_of(me * shard, shard), shard)
    fills = [
        pltpu.make_async_copy(src, dst, local_sem.at[i])
        for i, (src, dst) in enumerate((
            (wk, wkv_all.at[mine, pl.ds(0, cols)]),
            (wv, wkv_all.at[mine, pl.ds(cols, cols)]),
            (wq, wq_all.at[mine]),
            (wo, wo_own),
        ))
    ]
    loads = [
        pltpu.make_async_copy(tokens.at[pl.ds(c * chunk, chunk)], toks.at[pl.ds(c * chunk, chunk)],
                              tok_sem.at[c])
        for c in range(parts)
    ]
    smalls = [
        pltpu.make_async_copy(src, dst, small_sem.at[i])
        for i, (src, dst) in enumerate((
            (gain_in, gain), (freq_in, freq), (rates_in, rates), (out_gain_in, out_gain),
            (state_in, state_init)))
    ]
    barrier = pltpu.get_barrier_semaphore()

    def greet(device):
        pl.semaphore_signal(barrier, inc=1, device_id=device, device_id_type=MESH)

    greet(gq.device(z, y, 1 - x))
    greet(gq.device(z, 1 - y, x))
    for d in range(1, peers):
        greet((me, (tp + d) % peers))
    pl.when(z > 0)(lambda: greet(gq.device(z - 1, y, x)))
    pl.when(z < layers - 1)(lambda: greet(gq.device(z + 1, y, x)))

    for copy in fills + loads + smalls:
        copy.start()

    out_shard = wo.shape[1]
    for fill in fills[:3]:
        fill.wait()
    with SCOPE("barrier"):
        pl.semaphore_wait(
            barrier, 1 + peers + jnp.minimum(z, 1) + jnp.minimum(layers - 1 - z, 1))

    gk.lead()
    gk.spread(0)

    base = pl.multiple_of(tp * rows_here, rows_here)
    tile = min(64, chunk)

    def send_normed(d, c):
        ref = normed.at[pl.ds(pl.multiple_of(base + c * chunk, chunk), chunk)]
        return remote(ref, ref, nrm_s.at[d - 1], nrm_r.at[d - 1], (me, (tp + d) % peers))

    for copy in smalls:
        copy.wait()
    def sent_normed(d):
        ref = normed.at[pl.ds(base, rows_here)]
        return remote(ref, ref, nrm_s.at[d - 1], nrm_r.at[d - 1], (me, (tp + d) % peers))

    for c in range(parts):
        loads[c].wait()

        @pl.loop(c * chunk // tile, (c + 1) * chunk // tile)
        def _(i):
            at = pl.ds(pl.multiple_of(i * tile, tile), tile)
            u = toks[at, :].astype(F32)
            scale = lax.rsqrt(jnp.mean(u * u, axis=-1, keepdims=True) + EPS)
            normed[pl.ds(pl.multiple_of(base + i * tile, tile), tile), :] = (
                u * scale * gain[...]
            ).astype(BF16)

        for d in range(1, peers):
            send_normed(d, c).start()

    fills[3].wait()
    wo_all[pl.ds(pl.multiple_of(me * out_shard, out_shard), out_shard), :] = wo_own[...].T

    def trig(i, carry):
        at = pl.ds(pl.multiple_of(i * BLOCK, BLOCK), BLOCK)
        pos = lax.broadcasted_iota(jnp.int32, (BLOCK, HEAD_DIM), 0) + (me * span + i * BLOCK)
        angle = pos.astype(F32) * freq[...]
        lane = lax.broadcasted_iota(jnp.int32, (BLOCK, HEAD_DIM), 1)
        sin = jnp.sin(angle)
        cosine[at, :] = jnp.cos(angle)
        sine[at, :] = jnp.where(lane < HEAD_DIM // 2, -sin, sin)
        return carry

    deep = 4 * shard
    m_tile = min(256, span)

    def product(gather, t, n, first, count):
        with SCOPE("arrive"):
            for i in range(n):
                zi = gather.arrive(t + i)
        at_k = pl.ds(pl.multiple_of((zi // n) * (n * deep), n * deep), n * deep)
        with SCOPE("product"):
            @pl.loop(0, span // m_tile)
            def _(i):
                at = pl.ds(pl.multiple_of(i * m_tile, m_tile), m_tile)
                for c in range(count):
                    term = jnp.dot(normed[at, at_k], gather.buf[at_k, c * cols:(c + 1) * cols],
                                   preferred_element_type=F32)
                    at_c = pl.ds((first + c) * cols, cols)
                    acc[at, at_c] = term if t == 0 else acc[at, at_c] + term

    gap = (lax.broadcasted_iota(jnp.int32, (BLOCK, BLOCK), 0)
           - lax.broadcasted_iota(jnp.int32, (BLOCK, BLOCK), 1)).astype(F32)
    row = lax.broadcasted_iota(jnp.int32, (BLOCK, HEAD_DIM), 0).astype(F32)

    def states(b, sums):
        at = pl.ds(pl.multiple_of(b * BLOCK, BLOCK), BLOCK)
        cos, sin = cosine[at, :], sine[at, :]
        new = []
        for h in range(heads):
            rate = rates[h, b]
            head = pl.ds(h * HEAD_DIM, HEAD_DIM)
            u = acc[at, pl.ds(cols + h * HEAD_DIM, HEAD_DIM)]
            k = (u * cos + pltpu.roll(u, HEAD_DIM // 2, 1) * sin).astype(BF16)
            v = acc[at, pl.ds(2 * cols + h * HEAD_DIM, HEAD_DIM)].astype(BF16)
            k_rot[at, head] = k
            v_row[at, head] = v
            tail = jnp.exp(-(BLOCK - 1.0 - row) * rate) * HEAD_DIM ** (-0.5)
            kv = tn_dot((k.astype(F32) * tail).astype(BF16), v)
            now = state[h]
            prev[b, h] = now
            state[h] = jnp.exp(jnp.full((1, HEAD_DIM), -float(BLOCK), F32) * rate) * now + kv
            new.append(sums[h] + rate)
        return tuple(new)

    def decay_of(total):
        return jnp.exp(jnp.full((1, HEAD_DIM), -float(BLOCK), F32) * total)

    corner = 2 * y + x
    slots = max(heads // 4, 1)
    owner = None if heads >= 4 else corner < heads

    def toward(r):
        return (y + r // 2 - 2 * y * (r // 2)) * 2 + (x + r % 2 - 2 * x * (r % 2))

    def guard(r, act):
        act() if heads >= 4 else pl.when(toward(r) < heads)(act)

    def beside(r):
        return (4 * z + toward(r), tp)

    def total_to(r, i):
        return remote(tot_send.at[4 * i + toward(r)], tot_recv.at[i, r], t_s.at[i], t_r.at[i], beside(r))

    def plane_to(k, i):
        return remote(pl_send.at[i], pl_recv.at[i, z], p_s.at[i, k], p_r.at[i, z], (4 * (z + k) + corner, tp))

    def plane_from(zz, i):
        return remote(pl_send.at[i], pl_recv.at[i, zz], p_s.at[i, 0], p_r.at[i, zz], (4 * z + corner, tp))

    def start_to(r, i):
        return remote(in_send.at[i, r], in_recv.at[i, r], i_s.at[i], i_r.at[i], beside(r))

    def all_three(ref, send, recv):
        return remote(ref, ref, send, recv, beside(1))

    def packed(decay, value):
        return jnp.concatenate([value, jnp.broadcast_to(decay, (16, HEAD_DIM))], axis=0).astype(BF16)

    def opened(ref):
        return ref[HEAD_DIM:, :].astype(F32)[:1], ref[:HEAD_DIM, :].astype(F32)

    def mine_only(act):
        act() if heads >= 4 else pl.when(owner)(act)

    def send_totals():
        for h in range(heads):
            tot_send[h] = packed(decay_of(sums[h]), state[h])
        for r in (3, 1, 2):
            def go_out():
                for i in range(slots):
                    total_to(r, i).start()
            guard(r, go_out)

    def plane_totals():
        def act():
            for i in range(slots):
                tot_recv[i, 0] = tot_send[4 * i + corner]
                all_three(tot_recv.at[i, pl.ds(1, 3)], t_s.at[i], t_r.at[i]).wait_recv()
                decay, value = jnp.ones((1, HEAD_DIM), F32), jnp.zeros((HEAD_DIM, HEAD_DIM), F32)
                for j in range(4):
                    excl[i, j], excl_d[i, j] = value, jnp.broadcast_to(decay, (8, HEAD_DIM))
                    d, v = opened(tot_recv.at[i, toward(j)])
                    decay, value = decay * d, value * d + v
                pl_send[i] = packed(decay, value)
                for k in range(1, layers):
                    @pl.when(z + k < layers)
                    def _():
                        plane_to(k, i).start()
        mine_only(act)

    def starts():
        def act():
            for i in range(slots):
                start[...] = state_init[4 * i + corner]
                for zz in range(layers - 1):
                    @pl.when(zz < z)
                    def _():
                        plane_from(zz, i).wait_recv()
                        d, v = opened(pl_recv.at[i, zz])
                        start[...] = start[...] * d + v
                for r in (3, 1, 2):
                    at = toward(r)
                    in_send[i, r] = (excl_d[i, at][:1] * start[...] + excl[i, at]).astype(BF16)
                    start_to(r, i).start()
                incoming[4 * i + corner] = excl_d[i, corner][:1] * start[...] + excl[i, corner]
        mine_only(act)

    def started():
        for i in range(slots):
            if heads >= 4:
                all_three(in_recv.at[i, pl.ds(1, 3)], i_s.at[i], i_r.at[i]).wait_recv()
            for r in (1, 2, 3):
                def act():
                    if heads < 4:
                        start_to(r, i).wait_recv()
                    incoming[4 * i + toward(r)] = in_recv[i, r].astype(F32)
                guard(r, act)

    def sent_states():
        for i in range(slots):
            if heads >= 4:
                all_three(tot_recv.at[i, pl.ds(1, 3)], t_s.at[i], t_r.at[i]).wait_send()
            else:
                for r in (1, 2, 3):
                    guard(r, total_to(r, i).wait_send)

            def act():
                all_three(in_recv.at[i, pl.ds(1, 3)], i_s.at[i], i_r.at[i]).wait_send()
                for k in range(1, layers):
                    pl.when(z + k < layers)(plane_to(k, i).wait_send)
            mine_only(act)

    def turned(t):
        with SCOPE("arrive"):
            zi = gq.arrive(t)
        at_k = pl.ds(pl.multiple_of(zi * deep, deep), deep)
        with SCOPE("turned"):
            @pl.loop(0, span // m_tile)
            def _(i):
                at = pl.ds(pl.multiple_of(i * m_tile, m_tile), m_tile)
                u_all = acc[at, :cols] + jnp.dot(
                    normed[at, at_k], gq.buf[at_k, :], preferred_element_type=F32)
                cos, sin = cosine[at, :], sine[at, :]
                for h in range(heads):
                    u = u_all[:, h * HEAD_DIM:(h + 1) * HEAD_DIM]
                    q = u * cos + pltpu.roll(u, HEAD_DIM // 2, 1) * sin
                    q_rot[at, h * HEAD_DIM:(h + 1) * HEAD_DIM] = q.astype(BF16)
                    for n in range(m_tile // BLOCK):
                        read = jnp.exp(-(row + 1.0) * rates[h, i * (m_tile // BLOCK) + n])
                        at_b = pl.ds(pl.multiple_of(i * m_tile + n * BLOCK, BLOCK), BLOCK)
                        weigh[at_b, (2 * h + 1) * HEAD_DIM:(2 * h + 2) * HEAD_DIM] = (
                            q[n * BLOCK:(n + 1) * BLOCK] * read).astype(BF16)

    def scores(b, carry):
        at = pl.ds(pl.multiple_of(b * BLOCK, BLOCK), BLOCK)
        for h in range(heads):
            head = pl.ds(h * HEAD_DIM, HEAD_DIM)
            fall = jnp.where(gap >= 0.0, jnp.exp(-jnp.maximum(gap, 0.0) * rates[h, b]), 0.0)
            score = nt_dot(q_rot[at, head], k_rot[at, head]) * (fall * HEAD_DIM ** (-0.5))
            weigh[at, 2 * h * HEAD_DIM:(2 * h + 1) * HEAD_DIM] = score.astype(BF16)
        return carry

    def finish(b, sums):
        at = pl.ds(pl.multiple_of(b * BLOCK, BLOCK), BLOCK)
        new = []
        for h in range(heads):
            head = pl.ds(h * HEAD_DIM, HEAD_DIM)
            before = prev[b, h] + decay_of(sums[h]) * incoming[h]
            kept = jnp.dot(weigh[at, 2 * h * HEAD_DIM:(2 * h + 2) * HEAD_DIM],
                           jnp.concatenate([v_row[at, head], before.astype(BF16)], axis=0),
                           preferred_element_type=F32)
            kept = kept * lax.rsqrt(jnp.mean(kept * kept, axis=-1, keepdims=True) + EPS)
            hidden[at, head] = (kept * out_gain[:, head]).astype(BF16)
            new.append(sums[h] + rates[h, b])
        return tuple(new)

    wide = 4 * out_shard

    half_rows = rows_here // 2

    def hand(d, t, part_no=None):
        src, dst, k = part.at[d - 1, t], landed.at[d - 1, t], 2 * t
        if part_no is not None:
            rows = pl.ds(part_no * half_rows, half_rows)
            src, dst, k = src.at[rows], dst.at[rows], 2 * t + part_no
        return remote(src, dst, part_s.at[d - 1], part_r.at[d - 1, k], (me, (tp + d) % peers))

    def handed(t):
        return (0, 1) if t % 2 else (None,)

    def pieces(t):
        with SCOPE("oarrive"):
            zi = go.arrive(t)
        return pl.ds(pl.multiple_of(zi * wide, wide), wide)

    def theirs(t):
        rows_o = pieces(t)
        with SCOPE("theirs"):
            for n in handed(t):
                count = rows_here if n is None else half_rows
                for d in range(1, peers):
                    start = ((tp + d) % peers) * rows_here + (n or 0) * half_rows
                    rows = pl.ds(pl.multiple_of(start, count), count)
                    part[d - 1, t, pl.ds((n or 0) * half_rows, count), :] = nt_dot(
                        hidden[rows, :], wo_all[rows_o, :]).astype(BF16)
                    hand(d, t, n).start()

    def ours(t):
        at_c = pl.ds(pl.multiple_of(go.layer(t) * wide, wide), wide)
        for n in handed(t):
            count = rows_here if n is None else half_rows
            with SCOPE("w_hand"):
                for d in range(1, peers):
                    hand(d, t, n).wait_recv()
            with SCOPE("ours"):
                at = pl.ds((n or 0) * half_rows, count)
                rows = pl.ds(pl.multiple_of(base + (n or 0) * half_rows, count), count)
                value = nt_dot(hidden[rows, :], wo_all[at_c, :])
                for d in range(1, peers):
                    value = value + landed[d - 1, t, at, :].astype(F32)
                out[at, at_c] = value.astype(BF16)

    def sc(name, fn, *args):
        with SCOPE(name):
            fn(*args)

    evens, odds, last = range(2, layers, 2), range(1, layers - 2, 2), layers - 1
    cut = max(1, blocks // 2)

    def each(name, ts, fn):
        for t in ts:
            sc(name, fn, t)

    sc("kcross0", gk.cross, 0)
    sc("kstage1a", gk.stage, 1, (0,))
    sc("trig", lambda: lax.fori_loop(0, cut, trig, 0))
    sc("kstage1b", gk.stage, 1, (1,))
    each("kspread", odds, gk.spread)
    sc("trig", lambda: lax.fori_loop(cut, blocks, trig, 0))
    with SCOPE("nrmwait"):
        for d in range(1, peers):
            sent_normed(d).wait_recv()
    sc("kstage2a", gk.stage, 2, (0,))
    sc("kstage2b", gk.stage, 2, (1,))
    each("kspread", evens, gk.spread)
    sc("kswap0", gk.swap, 0)
    gq.lead(False)
    product(gk, 0, 1, 1, 2)
    each("kcross2", evens, gk.cross)
    gq.spread(0)
    sc("kstage3", gk.stage, 3)
    gk.spread(last)
    sc("qmiddle", gq.middle, 1, 2)
    each("kswap2", evens, gk.swap)
    for t in evens:
        product(gk, t, 1, 1, 2)
    sc("qmiddle3", gq.middle, 3)
    sc("qouter2", gq.outer, 2)
    gq.lead(True)
    each("qspread", evens, gq.spread)
    for t in odds:
        product(gk, t, 1, 1, 2)
    sc("qcross0", gq.cross, 0)
    go.lead(False)
    go.spread(0)
    product(gk, last, 1, 1, 2)

    for h in range(heads):
        state[h] = jnp.zeros((HEAD_DIM, HEAD_DIM), F32)
    with SCOPE("states"):
        sums = lax.fori_loop(0, cut, states, (jnp.float32(0.0),) * heads)
    each("qcross2", evens, gq.cross)
    sc("omiddle", go.middle, 1, 2)
    with SCOPE("states"):
        sums = lax.fori_loop(cut, blocks, states, sums)
    sc("send_tot", send_totals)
    sc("qswap0", gq.swap, 0)
    sc("qouter3", gq.outer, 3)
    sc("qouter1", gq.outer, 1)
    each("qspread", odds, gq.spread)
    gq.spread(last)
    product(gq, 0, 1, 0, 1)
    each("qswap2", evens, gq.swap)
    sc("plane_tot", plane_totals)
    sc("omiddle3", go.middle, 3)
    sc("oouter2", go.outer, 2)
    go.lead(True)
    each("ospread", evens, go.spread)
    sc("ocross0", go.cross, 0)
    for t in evens:
        product(gq, t, 1, 0, 1)
    for t in odds:
        product(gq, t, 1, 0, 1)
    sc("starts", starts)
    turned(last)
    each("ocross2", evens, go.cross)
    sc("oouter3", go.outer, 3)
    go.spread(last)
    with SCOPE("scores"):
        lax.fori_loop(0, cut, scores, 0)
    sc("oouter1", go.outer, 1)
    each("ospread", odds, go.spread)
    sc("oswap0", go.swap, 0)
    with SCOPE("scores"):
        lax.fori_loop(cut, blocks, scores, 0)
    sc("started", started)
    with SCOPE("finish"):
        sums = lax.fori_loop(0, cut, finish, (jnp.float32(0.0),) * heads)
    each("oswap2", evens, go.swap)
    with SCOPE("finish"):
        lax.fori_loop(cut, blocks, finish, sums)
    first, rest = (0,) + tuple(evens), tuple(odds) + (last,)

    def project(order):
        for turn, fn in order:
            for t in turn:
                fn(t)

    pl.when(tp % 2 == 0)(lambda: project(((first, theirs), (first, ours), (rest, theirs), (rest, ours))))
    pl.when(tp % 2 == 1)(lambda: project(((first, theirs), (rest, theirs), (first, ours), (rest, ours))))

    with SCOPE("drain"):
        gk.drain()
        gq.drain()
        go.drain()
        for d in range(1, peers):
            sent_normed(d).wait_send()
            remote(part.at[d - 1], landed.at[d - 1], part_s.at[d - 1], part_r.at[d - 1, 0],
                   (me, (tp + d) % peers)).wait_send()
        sent_states()


def shards(tokens, norm_gain, w_query, w_key, w_value, decay_rate, state_init, out_gain, w_out):
    n_sp, peers = lax.axis_size("sp"), lax.axis_size("tp")
    layers = n_sp // 4
    rows_here, width = tokens.shape
    span = rows_here * peers
    cols = w_query.shape[1]
    heads = cols // HEAD_DIM
    blocks = span // BLOCK
    half = HEAD_DIM // 2
    wide = 4 * w_out.shape[1]
    freq = ROPE_BASE ** (-np.arange(half, dtype=np.float64) / half)
    freq = np.concatenate([freq, freq])[None].astype(np.float32)
    vmem = pl.BlockSpec(memory_space=pltpu.VMEM)
    hbm = pl.BlockSpec(memory_space=pl.ANY)
    dma = pltpu.SemaphoreType.DMA
    others, slots = max(peers - 1, 1), max(heads // 4, 1)
    parts = 2
    gather_sems = [dma((layers // 2, 6)), dma((layers, 1)), dma((2,))]
    v = pltpu.VMEM
    return pl.pallas_call(
        functools.partial(kernel, layers, peers),
        out_shape=jax.ShapeDtypeStruct((rows_here, width), BF16),
        in_specs=[hbm] * 10,
        out_specs=vmem,
        scratch_shapes=[
            v((1, width), F32), pltpu.SMEM((heads, blocks), F32), v((heads, HEAD_DIM, HEAD_DIM), F32),
            v((1, cols), F32), v((1, HEAD_DIM), F32), dma((5,)),
            v((width, 2 * cols), BF16), v((width, cols), BF16), v((width, cols), BF16),
            v(w_out.shape, BF16), v((rows_here, width), BF16),
            v((span, width), BF16),
            v((span, 3 * cols), F32), v((span, HEAD_DIM), F32), v((span, HEAD_DIM), F32),
            v((span, cols), BF16), v((span, cols), BF16), v((span, cols), BF16), v((span, 2 * cols), BF16),
            v((blocks, heads, HEAD_DIM, HEAD_DIM), F32),
            v((heads, HEAD_DIM, HEAD_DIM), F32), v((span, cols), BF16),
            v((others, layers, rows_here, wide), BF16), v((others, layers, rows_here, wide), BF16),
            v((heads, HEAD_DIM + 16, HEAD_DIM), BF16), v((slots, 4, HEAD_DIM + 16, HEAD_DIM), BF16),
            v((slots, 4, HEAD_DIM, HEAD_DIM), F32), v((slots, 4, 8, HEAD_DIM), F32),
            v((slots, HEAD_DIM + 16, HEAD_DIM), BF16), v((slots, layers, HEAD_DIM + 16, HEAD_DIM), BF16),
            v((slots, 4, HEAD_DIM, HEAD_DIM), BF16), v((slots, 4, HEAD_DIM, HEAD_DIM), BF16),
            v((HEAD_DIM, HEAD_DIM), F32), v((heads, HEAD_DIM, HEAD_DIM), F32),
            dma((4,)), dma((parts,)), dma((others,)), dma((others,)),
            dma((others,)), dma((others, 2 * layers)),
            dma((slots,)), dma((slots,)), dma((slots, layers)), dma((slots, layers)),
            dma((slots,)), dma((slots,)),
        ] + [gather_sems[0], dma((layers, 2)), gather_sems[2]] + gather_sems * 2,
        compiler_params=pltpu.CompilerParams(
            collective_id=0, has_side_effects=True, vmem_limit_bytes=46 * 1024 * 1024),
    )(*(pltpu.with_memory_space_constraint(u, pltpu.HBM) for u in (
        tokens, norm_gain[None], w_query, w_key, w_value, w_out, decay_rate.T, state_init,
        out_gain[None], jnp.asarray(freq))))


def solution(mesh):
    in_specs = (
        P(("sp", "tp"), None),
        P(),
        P("sp", "tp"),
        P("sp", "tp"),
        P("sp", "tp"),
        P("sp", "tp"),
        P("tp", None, None),
        P("tp"),
        P("tp", "sp"),
    )
    out_specs = P(("sp", "tp"), None)
    return jax.shard_map(shards, mesh=mesh, in_specs=in_specs, out_specs=out_specs, check_vma=False)
```

```python
import functools

import jax
import jax.numpy as jnp
import numpy as np
from jax import lax
from jax.experimental import pallas as pl
from jax.experimental.pallas import tpu as pltpu
from jax.sharding import PartitionSpec as P

HEAD_DIM = 128
BLOCK = 128
EPS = 0.1
ROPE_BASE = 10000.0
MESH = pl.DeviceIdType.MESH
F32 = jnp.float32
BF16 = jnp.bfloat16


def remote(src, dst, send, recv, device):
    return pltpu.make_async_remote_copy(
        src_ref=src, dst_ref=dst, send_sem=send, recv_sem=recv, device_id=device, device_id_type=MESH
    )


class Gather:
    def __init__(self, buf, layers, place, sems, split=False):
        self.buf, self.layers, self.place = buf, layers, place
        self.pieces = (0, 1) if split else (None,)
        self.z, self.y, self.x, self.tp = place
        self.rows = buf.shape[0] // (4 * layers)
        self.got, self.r_z, self.sent = sems
        self.inner = (self.z > 0) & (self.z < layers - 1)

    def at(self, zi, yi, xi, piece=None):
        start = ((zi * 2 + yi) * 2 + xi) * self.rows
        if piece is None:
            return self.buf.at[pl.ds(pl.multiple_of(start, self.rows), self.rows)]
        half = self.rows // 2
        return self.buf.at[pl.ds(pl.multiple_of(start + piece * half, half), half)]

    def device(self, zi, yi, xi):
        return ((zi * 2 + yi) * 2 + xi, self.tp)

    def layer(self, t):
        zi, bit = self.z, 1
        while bit < self.layers:
            if t & bit:
                zi = zi + bit - 2 * bit * ((self.z // bit) % 2)
            bit *= 2
        return zi

    def copy_x(self, t, j):
        ref = self.at(self.layer(t), 1 - self.y if j == 2 else self.y, self.x, (0, 1, 0, None)[j])
        return remote(ref, ref, self.sent.at[0], self.got.at[t // 2, (2, 0, 1, 3)[j]],
                      self.device(self.z, self.y, 1 - self.x))

    def copy_y(self, t, j):
        ref = self.at(self.layer(t), self.y, 1 - self.x if j == 2 else self.x, (1, 0, 1, None)[j])
        return remote(ref, ref, self.sent.at[0], self.got.at[t // 2, (2, 0, 1, 3)[j]],
                      self.device(self.z, 1 - self.y, self.x))

    def copy_w(self, t):
        ref = self.at(self.layer(t), 1 - self.y, 1 - self.x)
        return remote(ref, ref, self.sent.at[0], self.got.at[t // 2, 4],
                      self.device(self.layer(1), self.y, self.x))

    def whole(self, t, shards, k):
        ref = self.buf.at[pl.ds(0, shards * self.rows)]
        remote(ref, ref, self.sent.at[0], self.got.at[t // 2, k],
               self.device(self.z, self.y, 1 - self.x)).wait_recv()

    def copy_z(self, zi, step, piece):
        ref = self.at(zi, self.y, self.x, piece)
        return remote(ref, ref, self.sent.at[1], self.r_z.at[zi, piece or 0],
                      self.device(self.z + step, self.y, self.x))

    def order(self, t):
        z, last = self.z, self.layers - 1
        near = z - (t + 1) // 2 if t % 2 else z + t // 2
        m = jnp.minimum(z, last - z)
        far = jnp.where(z < last - z, t, last - t)
        return jnp.where(t <= 2 * m, near, far)

    def along(self, zi, piece):
        @pl.when((zi <= self.z) & (self.z < self.layers - 1))
        def _():
            self.copy_z(zi, 1, piece).start()

        @pl.when((zi >= self.z) & (self.z > 0))
        def _():
            self.copy_z(zi, -1, piece).start()

    def lead(self, late=None):
        for piece in self.pieces:
            if late is None or self.layers != 4:
                if not late:
                    self.along(self.z, piece)
                continue
            even, outer = self.z % 2 == 0, jnp.logical_not(self.inner)
            odd = jnp.logical_not(even)
            up = self.inner & even if late else (self.z < self.layers - 1) & (outer | odd)
            down = self.inner & odd if late else (self.z > 0) & (outer | even)
            pl.when(up)(lambda: self.copy_z(self.z, 1, piece).start())
            pl.when(down)(lambda: self.copy_z(self.z, -1, piece).start())

    def take(self, t, pieces, when=None):
        zi = self.order(t)

        def go():
            for piece in pieces:
                self.copy_z(zi, 1, piece).wait_recv()
                self.along(zi, piece)

        go() if when is None else pl.when(when)(go)

    def stage(self, s, pieces=None):
        pieces = pieces or self.pieces
        if self.layers != 4:
            if s == 1:
                for t in range(1, self.layers):
                    self.take(t, pieces)
            return
        if s == 1:
            self.take(1, pieces)
            self.take(2, pieces, self.inner)
        elif s == 2:
            self.take(2, pieces, jnp.logical_not(self.inner))
            self.take(3, pieces, self.inner)
        else:
            self.take(3, pieces, jnp.logical_not(self.inner))

    def middle(self, *order):
        if self.layers == 4:
            for t in order:
                self.take(t, self.pieces, self.inner)
        elif 1 in order:
            for t in range(1, self.layers):
                self.take(t, self.pieces)

    def outer(self, *order):
        if self.layers == 4:
            for t in order:
                self.take(t, self.pieces, jnp.logical_not(self.inner))

    def spread(self, t):
        if t % 2:
            self.copy_x(t, 3).start()
            self.copy_y(t, 3).start()
            return
        self.copy_y(t, 1).start()
        self.copy_x(t, 1).start()
        self.copy_x(t, 0).start()
        self.copy_y(t, 0).start()

    def cross(self, t):
        self.whole(t, 1, 0)
        self.copy_x(t, 2).start()
        self.copy_y(t, 2).start()

    def swap(self, t):
        self.whole(t, 1, 1)
        self.copy_w(t).start()

    def beside(self, t):
        self.whole(t, 2, 3)

    def across(self, t):
        self.whole(t, 1, 4)

    def arrive(self, t):
        if t % 2:
            self.beside(t)
            self.across(t)
        else:
            self.whole(t, 1, 2)
        return self.layer(t)

    def drain(self):
        def sent(k, shards):
            ref = self.buf.at[pl.ds(0, shards * self.rows)]
            remote(ref, ref, self.sent.at[k], self.r_z.at[0, 0], self.device(self.z, self.y, 1 - self.x)).wait_send()

        sent(0, 3 * self.layers)
        pl.when(self.inner)(lambda: sent(1, self.layers + 1))
        pl.when(jnp.logical_not(self.inner))(lambda: sent(1, 1))


def nt_dot(a, b):
    return lax.dot_general(a, b, (((1,), (1,)), ((), ())), preferred_element_type=F32)


def tn_dot(a, b):
    return lax.dot_general(a, b, (((0,), (0,)), ((), ())), preferred_element_type=F32)


SCOPE = jax.named_scope


def kernel(layers, peers, tokens, gain_in, wq, wk, wv, wo, rates_in, state_in, out_gain_in, freq_in, out,
           gain, rates, state_init, out_gain, freq, small_sem, wkv_all, wq_all, wo_all, wo_own, toks, normed, acc, cosine, sine, q_rot, k_rot, v_row, weigh,
           prev, state, hidden, cum, hid_peer, wo_peer, begun, tot_send, tot_recv, excl, excl_d, pl_send, pl_recv,
           in_send, in_recv, start, incoming, local_sem, tok_sem, nrm_s, nrm_r, hid_s, hid_r, wgt_s, wgt_r, t_s, t_r,
           p_s, p_r, i_s, i_r,
           *gather_sems):
    me, tp = lax.axis_index("sp"), lax.axis_index("tp")
    z, y, x = me // 4, (me // 2) % 2, me % 2
    rows_here, width = tokens.shape
    span = rows_here * peers
    cols = wq.shape[1]
    heads = cols // HEAD_DIM
    blocks = span // BLOCK
    shard = wq.shape[0]
    place = (z, y, x, tp)
    gk = Gather(wkv_all, layers, place, gather_sems[:3], True)
    gq = Gather(wq_all, layers, place, gather_sems[3:6])
    go = Gather(wo_all, layers, place, gather_sems[6:])
    parts = tok_sem.shape[0]
    chunk = rows_here // parts

    mine = pl.ds(pl.multiple_of(me * shard, shard), shard)
    fills = [
        pltpu.make_async_copy(src, dst, local_sem.at[i])
        for i, (src, dst) in enumerate((
            (wk, wkv_all.at[mine, pl.ds(0, cols)]),
            (wv, wkv_all.at[mine, pl.ds(cols, cols)]),
            (wq, wq_all.at[mine]),
            (wo, wo_own),
        ))
    ]
    loads = [
        pltpu.make_async_copy(tokens.at[pl.ds(c * chunk, chunk)], toks.at[pl.ds(c * chunk, chunk)],
                              tok_sem.at[c])
        for c in range(parts)
    ]
    smalls = [
        pltpu.make_async_copy(src, dst, small_sem.at[i])
        for i, (src, dst) in enumerate((
            (gain_in, gain), (freq_in, freq), (rates_in, rates), (out_gain_in, out_gain),
            (state_in, state_init)))
    ]
    for copy in fills[:2]:
        copy.start()
    barrier = pltpu.get_barrier_semaphore()

    def greet(device):
        pl.semaphore_signal(barrier, inc=1, device_id=device, device_id_type=MESH)

    greet(gq.device(z, y, 1 - x))
    greet(gq.device(z, 1 - y, x))
    for d in range(1, peers):
        greet((me, (tp + d) % peers))
    pl.when(z > 0)(lambda: greet(gq.device(z - 1, y, x)))
    pl.when(z < layers - 1)(lambda: greet(gq.device(z + 1, y, x)))

    for copy in fills[2:] + loads + smalls:
        copy.start()

    out_shard = wo.shape[1]
    for fill in fills[:2]:
        fill.wait()
    with SCOPE("barrier"):
        pl.semaphore_wait(
            barrier, 1 + peers + jnp.minimum(z, 1) + jnp.minimum(layers - 1 - z, 1))

    gk.lead()
    gk.spread(0)

    base = pl.multiple_of(tp * rows_here, rows_here)
    tile = min(64, chunk)

    def send_normed(d, c):
        ref = normed.at[pl.ds(pl.multiple_of(base + c * chunk, chunk), chunk)]
        return remote(ref, ref, nrm_s.at[d - 1], nrm_r.at[d - 1], (me, (tp + d) % peers))

    for copy in smalls:
        copy.wait()
    def sent_normed(d):
        ref = normed.at[pl.ds(base, rows_here)]
        return remote(ref, ref, nrm_s.at[d - 1], nrm_r.at[d - 1], (me, (tp + d) % peers))

    for c in range(parts):
        loads[c].wait()

        @pl.loop(c * chunk // tile, (c + 1) * chunk // tile)
        def _(i):
            at = pl.ds(pl.multiple_of(i * tile, tile), tile)
            u = toks[at, :].astype(F32)
            scale = lax.rsqrt(jnp.mean(u * u, axis=-1, keepdims=True) + EPS)
            normed[pl.ds(pl.multiple_of(base + i * tile, tile), tile), :] = (
                u * scale * gain[...]
            ).astype(BF16)

        for d in range(1, peers):
            send_normed(d, c).start()

    for fill in fills[2:]:
        fill.wait()
    wo_all[pl.ds(pl.multiple_of(me * out_shard, out_shard), out_shard), :] = wo_own[...].T

    def trig(i, carry):
        at = pl.ds(pl.multiple_of(i * BLOCK, BLOCK), BLOCK)
        pos = lax.broadcasted_iota(jnp.int32, (BLOCK, HEAD_DIM), 0) + (me * span + i * BLOCK)
        angle = pos.astype(F32) * freq[...]
        lane = lax.broadcasted_iota(jnp.int32, (BLOCK, HEAD_DIM), 1)
        sin = jnp.sin(angle)
        cosine[at, :] = jnp.cos(angle)
        sine[at, :] = jnp.where(lane < HEAD_DIM // 2, -sin, sin)
        return carry

    deep = 4 * shard
    m_tile = min(256, span)

    def product(gather, t, n, first, count):
        with SCOPE("arrive"):
            for i in range(n):
                zi = gather.arrive(t + i)
        at_k = pl.ds(pl.multiple_of((zi // n) * (n * deep), n * deep), n * deep)
        with SCOPE("product"):
            @pl.loop(0, span // m_tile)
            def _(i):
                at = pl.ds(pl.multiple_of(i * m_tile, m_tile), m_tile)
                for c in range(count):
                    term = jnp.dot(normed[at, at_k], gather.buf[at_k, c * cols:(c + 1) * cols],
                                   preferred_element_type=F32)
                    at_c = pl.ds((first + c) * cols, cols)
                    acc[at, at_c] = term if t == 0 else acc[at, at_c] + term

    gap = (lax.broadcasted_iota(jnp.int32, (BLOCK, BLOCK), 0)
           - lax.broadcasted_iota(jnp.int32, (BLOCK, BLOCK), 1)).astype(F32)
    row = lax.broadcasted_iota(jnp.int32, (BLOCK, HEAD_DIM), 0).astype(F32)

    def states(b, sums):
        at = pl.ds(pl.multiple_of(b * BLOCK, BLOCK), BLOCK)
        cos, sin = cosine[at, :], sine[at, :]
        new = []
        for h in range(heads):
            rate = rates[h, b]
            head = pl.ds(h * HEAD_DIM, HEAD_DIM)
            u = acc[at, pl.ds(cols + h * HEAD_DIM, HEAD_DIM)]
            k = (u * cos + pltpu.roll(u, HEAD_DIM // 2, 1) * sin).astype(BF16)
            v = acc[at, pl.ds(2 * cols + h * HEAD_DIM, HEAD_DIM)].astype(BF16)
            k_rot[at, head] = k
            v_row[at, head] = v
            tail = jnp.exp(-(BLOCK - 1.0 - row) * rate) * HEAD_DIM ** (-0.5)
            kv = tn_dot((k.astype(F32) * tail).astype(BF16), v)
            now = state[h]
            prev[b, h] = now
            state[h] = jnp.exp(jnp.full((1, HEAD_DIM), -float(BLOCK), F32) * rate) * now + kv
            cum[h, b] = sums[h]
            new.append(sums[h] + rate)
        return tuple(new)

    def decay_of(total):
        return jnp.exp(jnp.full((1, HEAD_DIM), -float(BLOCK), F32) * total)

    corner = 2 * y + x
    slots = max(heads // 4, 1)
    owner = None if heads >= 4 else corner < heads

    def toward(r):
        return (y + r // 2 - 2 * y * (r // 2)) * 2 + (x + r % 2 - 2 * x * (r % 2))

    def guard(r, act):
        act() if heads >= 4 else pl.when(toward(r) < heads)(act)

    def beside(r):
        return (4 * z + toward(r), tp)

    def total_to(r, i):
        return remote(tot_send.at[4 * i + toward(r)], tot_recv.at[i, r], t_s.at[i], t_r.at[i], beside(r))

    def plane_to(k, i):
        return remote(pl_send.at[i], pl_recv.at[i, z], p_s.at[i], p_r.at[i, z], (4 * (z + k) + corner, tp))

    def plane_from(zz, i):
        return remote(pl_send.at[i], pl_recv.at[i, zz], p_s.at[i], p_r.at[i, zz], (4 * z + corner, tp))

    def start_to(r, i):
        return remote(in_send.at[i, r], in_recv.at[i, r], i_s.at[i], i_r.at[i], beside(r))

    def all_three(ref, send, recv):
        return remote(ref, ref, send, recv, beside(1))

    def packed(decay, value):
        return jnp.concatenate([value, jnp.broadcast_to(decay, (16, HEAD_DIM))], axis=0).astype(BF16)

    def opened(ref):
        return ref[HEAD_DIM:, :].astype(F32)[:1], ref[:HEAD_DIM, :].astype(F32)

    def mine_only(act):
        act() if heads >= 4 else pl.when(owner)(act)

    def send_totals():
        for h in range(heads):
            tot_send[h] = packed(decay_of(sums[h]), state[h])
        for r in (3, 1, 2):
            def go_out():
                for i in range(slots):
                    total_to(r, i).start()
            guard(r, go_out)

    def plane_totals():
        def act():
            for i in range(slots):
                tot_recv[i, 0] = tot_send[4 * i + corner]
                all_three(tot_recv.at[i, pl.ds(1, 3)], t_s.at[i], t_r.at[i]).wait_recv()
                decay, value = jnp.ones((1, HEAD_DIM), F32), jnp.zeros((HEAD_DIM, HEAD_DIM), F32)
                for j in range(4):
                    excl[i, j], excl_d[i, j] = value, jnp.broadcast_to(decay, (8, HEAD_DIM))
                    d, v = opened(tot_recv.at[i, toward(j)])
                    decay, value = decay * d, value * d + v
                pl_send[i] = packed(decay, value)
                for k in range(1, layers):
                    @pl.when(z + k < layers)
                    def _():
                        plane_to(k, i).start()
        mine_only(act)

    def starts():
        def act():
            for i in range(slots):
                start[...] = state_init[4 * i + corner]
                for zz in range(layers - 1):
                    @pl.when(zz < z)
                    def _():
                        plane_from(zz, i).wait_recv()
                        d, v = opened(pl_recv.at[i, zz])
                        start[...] = start[...] * d + v
                for r in (3, 1, 2):
                    at = toward(r)
                    in_send[i, r] = (excl_d[i, at][:1] * start[...] + excl[i, at]).astype(BF16)
                    start_to(r, i).start()
                incoming[4 * i + corner] = excl_d[i, corner][:1] * start[...] + excl[i, corner]
        mine_only(act)

    def started():
        for i in range(slots):
            if heads >= 4:
                all_three(in_recv.at[i, pl.ds(1, 3)], i_s.at[i], i_r.at[i]).wait_recv()
            for r in (1, 2, 3):
                def act():
                    if heads < 4:
                        start_to(r, i).wait_recv()
                    incoming[4 * i + toward(r)] = in_recv[i, r].astype(F32)
                guard(r, act)

    def sent_states():
        for i in range(slots):
            if heads >= 4:
                all_three(tot_recv.at[i, pl.ds(1, 3)], t_s.at[i], t_r.at[i]).wait_send()
            else:
                for r in (1, 2, 3):
                    guard(r, total_to(r, i).wait_send)

            def act():
                all_three(in_recv.at[i, pl.ds(1, 3)], i_s.at[i], i_r.at[i]).wait_send()
                for zz in range(layers - 1):
                    ref = pl_recv.at[i, pl.ds(0, layers - 1 - zz)]
                    pl.when(z == zz)(all_three(ref, p_s.at[i], p_r.at[i, 0]).wait_send)
            mine_only(act)

    def turned(t):
        with SCOPE("arrive"):
            zi = gq.arrive(t)
        at_k = pl.ds(pl.multiple_of(zi * deep, deep), deep)
        with SCOPE("turned"):
            @pl.loop(0, span // m_tile)
            def _(i):
                at = pl.ds(pl.multiple_of(i * m_tile, m_tile), m_tile)
                u_all = acc[at, :cols] + jnp.dot(
                    normed[at, at_k], gq.buf[at_k, :], preferred_element_type=F32)
                cos, sin = cosine[at, :], sine[at, :]
                for h in range(heads):
                    u = u_all[:, h * HEAD_DIM:(h + 1) * HEAD_DIM]
                    q = u * cos + pltpu.roll(u, HEAD_DIM // 2, 1) * sin
                    q_rot[at, h * HEAD_DIM:(h + 1) * HEAD_DIM] = q.astype(BF16)
                    for n in range(m_tile // BLOCK):
                        read = jnp.exp(-(row + 1.0) * rates[h, i * (m_tile // BLOCK) + n])
                        at_b = pl.ds(pl.multiple_of(i * m_tile + n * BLOCK, BLOCK), BLOCK)
                        weigh[at_b, (2 * h + 1) * HEAD_DIM:(2 * h + 2) * HEAD_DIM] = (
                            q[n * BLOCK:(n + 1) * BLOCK] * read).astype(BF16)

    def scores(b, carry):
        at = pl.ds(pl.multiple_of(b * BLOCK, BLOCK), BLOCK)
        for h in range(heads):
            head = pl.ds(h * HEAD_DIM, HEAD_DIM)
            fall = jnp.where(gap >= 0.0, jnp.exp(-jnp.maximum(gap, 0.0) * rates[h, b]), 0.0)
            score = nt_dot(q_rot[at, head], k_rot[at, head]) * (fall * HEAD_DIM ** (-0.5))
            weigh[at, 2 * h * HEAD_DIM:(2 * h + 1) * HEAD_DIM] = score.astype(BF16)
        return carry

    def finish(b, carry):
        at = pl.ds(pl.multiple_of(b * BLOCK, BLOCK), BLOCK)
        for h in range(heads):
            head = pl.ds(h * HEAD_DIM, HEAD_DIM)
            before = prev[b, h] + decay_of(cum[h, b]) * incoming[h]
            kept = jnp.dot(weigh[at, 2 * h * HEAD_DIM:(2 * h + 2) * HEAD_DIM],
                           jnp.concatenate([v_row[at, head], before.astype(BF16)], axis=0),
                           preferred_element_type=F32)
            kept = kept * lax.rsqrt(jnp.mean(kept * kept, axis=-1, keepdims=True) + EPS)
            hidden[at, head] = (kept * out_gain[:, head]).astype(BF16)
        return carry

    def finish_rows(owner_tp):
        start = owner_tp * (rows_here // BLOCK)
        lax.fori_loop(start, start + rows_here // BLOCK, finish, 0)

    wide = 4 * out_shard

    def columns(t):
        return pl.ds(pl.multiple_of(go.layer(t) * wide, wide), wide)

    def give_hidden(d):
        rows = pl.ds(pl.multiple_of(((tp + d) % peers) * rows_here, rows_here), rows_here)
        return remote(hidden.at[rows], hid_peer.at[d - 1], hid_s.at[d - 1], hid_r.at[d - 1],
                      (me, (tp + d) % peers))

    def give_weight(d, t):
        return remote(wo_all.at[columns(t)], wo_peer.at[d - 1, columns(t)], wgt_s.at[d - 1],
                      wgt_r.at[d - 1, t], (me, (tp + d) % peers))

    def forward(t):
        with SCOPE("oarrive"):
            go.arrive(t)
        for d in range(1, peers):
            give_weight(d, t).start()

    def give_shards(t, *corners):
        for yi, xi in corners:
            start = pl.multiple_of((4 * go.layer(t) + 2 * yi + xi) * out_shard, out_shard)
            rows = pl.ds(start, out_shard)
            for d in range(1, peers):
                remote(wo_all.at[rows], wo_peer.at[d - 1, rows], wgt_s.at[d - 1], wgt_r.at[d - 1, t],
                       (me, (tp + d) % peers)).start()

    def forward_own(t):
        give_shards(t, (y, x))

    def forward_beside(t):
        with SCOPE("w_beside"):
            go.beside(t)
        give_shards(t, (y, 1 - x), (1 - y, x))

    def forward_across(t):
        with SCOPE("w_across"):
            go.across(t)
        give_shards(t, (1 - y, 1 - x))

    def own_part(t):
        return nt_dot(hidden[pl.ds(base, rows_here), :], wo_all[columns(t), :])

    def peer_part(t, value):
        for d in range(1, peers):
            value = value + nt_dot(hid_peer[d - 1], wo_peer[d - 1, columns(t), :])
        return value

    def await_weight(t):
        with SCOPE("w_weight"):
            for d in range(1, peers):
                give_weight(d, t).wait_recv()

    def full(t):
        await_weight(t)
        with SCOPE("full"):
            out[:, columns(t)] = peer_part(t, own_part(t)).astype(BF16)

    def begin(t):
        with SCOPE("begin"):
            begun[t // 2] = own_part(t)

    def end(t):
        await_weight(t)
        with SCOPE("end"):
            out[:, columns(t)] = peer_part(t, begun[t // 2]).astype(BF16)

    def await_hidden():
        with SCOPE("w_hidden"):
            for d in range(1, peers):
                give_hidden(d).wait_recv()

    def sc(name, fn, *args):
        with SCOPE(name):
            fn(*args)

    evens, odds, last = range(2, layers, 2), range(1, layers - 2, 2), layers - 1
    cut = max(1, blocks // 2)

    def each(name, ts, fn):
        for t in ts:
            sc(name, fn, t)

    sc("kcross0", gk.cross, 0)
    sc("kstage1a", gk.stage, 1, (0,))
    sc("trig", lambda: lax.fori_loop(0, cut, trig, 0))
    sc("kstage1b", gk.stage, 1, (1,))
    each("kspread", odds, gk.spread)
    sc("trig", lambda: lax.fori_loop(cut, blocks, trig, 0))
    with SCOPE("nrmwait"):
        for d in range(1, peers):
            sent_normed(d).wait_recv()
    sc("kstage2a", gk.stage, 2, (0,))
    sc("kstage2b", gk.stage, 2, (1,))
    each("kspread", evens, gk.spread)
    sc("kswap0", gk.swap, 0)
    gq.lead(False)
    product(gk, 0, 1, 1, 2)
    each("kcross2", evens, gk.cross)
    gq.spread(0)
    sc("kstage3", gk.stage, 3)
    gk.spread(last)
    sc("qmiddle", gq.middle, 1, 2)
    each("kswap2", evens, gk.swap)
    for t in evens:
        product(gk, t, 1, 1, 2)
    sc("qmiddle3", gq.middle, 3)
    sc("qouter2", gq.outer, 2)
    gq.lead(True)
    each("qspread", evens, gq.spread)
    for t in odds:
        product(gk, t, 1, 1, 2)
    sc("qcross0", gq.cross, 0)
    go.lead(False)
    go.spread(0)
    product(gk, last, 1, 1, 2)

    for h in range(heads):
        state[h] = jnp.zeros((HEAD_DIM, HEAD_DIM), F32)
    with SCOPE("states"):
        sums = lax.fori_loop(0, cut, states, (jnp.float32(0.0),) * heads)
    each("qcross2", evens, gq.cross)
    sc("omiddle", go.middle, 1, 2)
    with SCOPE("states"):
        sums = lax.fori_loop(cut, blocks, states, sums)
    sc("send_tot", send_totals)
    sc("qswap0", gq.swap, 0)
    sc("qouter3", gq.outer, 3)
    sc("qouter1", gq.outer, 1)
    each("qspread", odds, gq.spread)
    gq.spread(last)
    product(gq, 0, 1, 0, 1)
    each("qswap2", evens, gq.swap)
    sc("plane_tot", plane_totals)
    sc("omiddle3", go.middle, 3)
    sc("oouter2", go.outer, 2)
    go.lead(True)
    each("ospread", evens, go.spread)
    sc("ocross0", go.cross, 0)
    for t in evens:
        product(gq, t, 1, 0, 1)
    for t in odds:
        product(gq, t, 1, 0, 1)
    sc("starts", starts)
    turned(last)
    each("ocross2", evens, go.cross)
    sc("oouter3", go.outer, 3)
    go.spread(last)
    forward_own(last)
    with SCOPE("scores"):
        lax.fori_loop(0, cut, scores, 0)
    sc("oouter1", go.outer, 1)
    each("ospread", odds, go.spread)
    each("ofwd", odds, forward_own)
    sc("oswap0", go.swap, 0)
    forward(0)
    with SCOPE("scores"):
        lax.fori_loop(cut, blocks, scores, 0)
    sc("started", started)
    with SCOPE("finish"):
        for d in range(1, peers):
            finish_rows((tp + d) % peers)
            give_hidden(d).start()
    for t in evens:
        sc("oswap2", go.swap, t)
        forward(t)
    with SCOPE("finish"):
        finish_rows(tp)
    first, rest = (0,) + tuple(evens), tuple(odds) + (last,)

    def project(early):
        def run(fn, ts):
            for t in ts:
                fn(t)

        if early:
            run(forward_beside, (last,))
            run(forward_across, odds)
            run(forward_beside, odds)
            run(forward_across, (last,))
        await_hidden()
        run(full, (0,))
        if not early:
            run(forward_beside, (last,))
            run(forward_across, odds)
        run(full, evens)
        if not early:
            run(forward_beside, odds)
        run(begin, odds)
        if not early:
            run(forward_across, (last,))
        run(begin, (last,))
        run(end, rest)

    pl.when(tp % 2 == 0)(lambda: project(False))
    pl.when(tp % 2 == 1)(lambda: project(True))

    with SCOPE("drain"):
        gk.drain()
        gq.drain()
        go.drain()
        for d in range(1, peers):
            sent_normed(d).wait_send()
            give_hidden(d).wait_send()
            remote(wo_all, wo_peer.at[d - 1], wgt_s.at[d - 1], wgt_r.at[d - 1, 0],
                   (me, (tp + d) % peers)).wait_send()
        sent_states()


def shards(tokens, norm_gain, w_query, w_key, w_value, decay_rate, state_init, out_gain, w_out):
    n_sp, peers = lax.axis_size("sp"), lax.axis_size("tp")
    layers = n_sp // 4
    rows_here, width = tokens.shape
    span = rows_here * peers
    cols = w_query.shape[1]
    heads = cols // HEAD_DIM
    blocks = span // BLOCK
    half = HEAD_DIM // 2
    wide = 4 * w_out.shape[1]
    freq = ROPE_BASE ** (-np.arange(half, dtype=np.float64) / half)
    freq = np.concatenate([freq, freq])[None].astype(np.float32)
    vmem = pl.BlockSpec(memory_space=pltpu.VMEM)
    hbm = pl.BlockSpec(memory_space=pl.ANY)
    dma = pltpu.SemaphoreType.DMA
    others, slots = max(peers - 1, 1), max(heads // 4, 1)
    parts = 2
    gather_sems = [dma((layers // 2, 5)), dma((layers, 1)), dma((2,))]
    v = pltpu.VMEM
    return pl.pallas_call(
        functools.partial(kernel, layers, peers),
        out_shape=jax.ShapeDtypeStruct((rows_here, width), BF16),
        in_specs=[hbm] * 10,
        out_specs=vmem,
        scratch_shapes=[
            v((1, width), F32), pltpu.SMEM((heads, blocks), F32), v((heads, HEAD_DIM, HEAD_DIM), F32),
            v((1, cols), F32), v((1, HEAD_DIM), F32), dma((5,)),
            v((width, 2 * cols), BF16), v((width, cols), BF16), v((width, cols), BF16),
            v(w_out.shape, BF16), v((rows_here, width), BF16),
            v((span, width), BF16),
            v((span, 3 * cols), F32), v((span, HEAD_DIM), F32), v((span, HEAD_DIM), F32),
            v((span, cols), BF16), v((span, cols), BF16), v((span, cols), BF16), v((span, 2 * cols), BF16),
            v((blocks, heads, HEAD_DIM, HEAD_DIM), F32),
            v((heads, HEAD_DIM, HEAD_DIM), F32), v((span, cols), BF16),
            pltpu.SMEM((heads, blocks), F32), v((others, rows_here, cols), BF16),
            v((others, width, cols), BF16), v((layers // 2, rows_here, wide), F32),
            v((heads, HEAD_DIM + 16, HEAD_DIM), BF16), v((slots, 4, HEAD_DIM + 16, HEAD_DIM), BF16),
            v((slots, 4, HEAD_DIM, HEAD_DIM), F32), v((slots, 4, 8, HEAD_DIM), F32),
            v((slots, HEAD_DIM + 16, HEAD_DIM), BF16), v((slots, layers, HEAD_DIM + 16, HEAD_DIM), BF16),
            v((slots, 4, HEAD_DIM, HEAD_DIM), BF16), v((slots, 4, HEAD_DIM, HEAD_DIM), BF16),
            v((HEAD_DIM, HEAD_DIM), F32), v((heads, HEAD_DIM, HEAD_DIM), F32),
            dma((4,)), dma((parts,)), dma((others,)), dma((others,)),
            dma((others,)), dma((others,)), dma((others,)), dma((others, layers)),
            dma((slots,)), dma((slots,)), dma((slots,)), dma((slots, layers)),
            dma((slots,)), dma((slots,)),
        ] + [gather_sems[0], dma((layers, 2)), gather_sems[2]] + gather_sems * 2,
        compiler_params=pltpu.CompilerParams(
            collective_id=0, has_side_effects=True, vmem_limit_bytes=46 * 1024 * 1024),
    )(*(pltpu.with_memory_space_constraint(u, pltpu.HBM) for u in (
        tokens, norm_gain[None], w_query, w_key, w_value, w_out, decay_rate.T, state_init,
        out_gain[None], jnp.asarray(freq))))


def solution(mesh):
    in_specs = (
        P(("sp", "tp"), None),
        P(),
        P("sp", "tp"),
        P("sp", "tp"),
        P("sp", "tp"),
        P("sp", "tp"),
        P("tp", None, None),
        P("tp"),
        P("tp", "sp"),
    )
    out_specs = P(("sp", "tp"), None)
    return jax.shard_map(shards, mesh=mesh, in_specs=in_specs, out_specs=out_specs, check_vma=False)
```
